128 devices in a mesh: fs: 16 (over z, y), tp: 8 (over x, core).
Axes of the slice: x: 4, y: 4, z: 4, core: 2. Of those that a mesh axis runs over, the one named last changes fastest.
Arguments:
- tokens: bfloat16 [12288, 2048], P('fs', 'tp'), may hold values from -40 to 40
- gain_one: float32 [2048], P('tp'), may hold values from 0.1 to 1.9
- w_gate: float32 [2048, 3072], P('fs', 'tp'), may hold values from -0.125 to 0.125
- w_up: float32 [2048, 3072], P('fs', 'tp'), may hold values from -0.125 to 0.125
- w_down: float32 [3072, 2048], P('tp', 'fs'), may hold values from -0.109375 to 0.109375
- scale_gate: float32 [3072], P('tp'), may hold values from 0.5 to 2
- scale_up: float32 [3072], P('tp'), may hold values from 0.5 to 2
- scale_down: float32 [2048], P('tp'), may hold values from 0.5 to 2
- gain_mix: float32 [2048], P('tp'), may hold values from 0.1 to 1.9
- w_query: float32 [2048, 2048], P('fs', 'tp'), may hold values from -0.125 to 0.125
- w_key: float32 [2048, 2048], P('fs', 'tp'), may hold values from -0.125 to 0.125
- w_value: float32 [2048, 2048], P('fs', 'tp'), may hold values from -0.125 to 0.125
- w_outgate: float32 [2048, 2048], P('fs', 'tp'), may hold values from -0.125 to 0.125
- scale_query: float32 [2048], P('tp'), may hold values from 0.5 to 2
- scale_key: float32 [2048], P('tp'), may hold values from 0.5 to 2
- scale_value: float32 [2048], P('tp'), may hold values from 0.5 to 2
- scale_outgate: float32 [2048], P('tp'), may hold values from 0.5 to 2
- ret_gain: float32 [2048], P('tp'), may hold values from 0.1 to 1.9
- decay_rate: float32 [8], P('tp'), may hold values from 0 to 2
- w_mix: float32 [2048, 2048], P('tp', 'fs'), may hold values from -0.125 to 0.125
- scale_mix: float32 [2048], P('tp'), may hold values from 0.5 to 2
- gain_two: float32 [2048], P('tp'), may hold values from 0.1 to 1.9
Outputs:
- layer_out: bfloat16 [12288, 2048], P('fs', 'tp')
The draws below stay inside these ranges and needn't reach their ends.
All inputs are finite; a program needn't handle non-finite values.
Results may differ from the reference program's by a relative error of at most 0.022.
Values may be sent and summed in bfloat16 or wider, within the bound.
A program may use at most 128 MiB of HBM per device.

```python
import math
import jax
import jax.numpy as jnp
from jax import lax

D = 2048
FF = 3072
HEADS = 8
LEN = 256
BLK = 128
RW = 2048
TOKENS = 12288
N_TP = 8


def draw_tokens(key, part):
    base = jax.random.normal(jax.random.fold_in(key, 13), (TOKENS, D), jnp.float32)
    logs = jax.random.uniform(jax.random.fold_in(key, 14), (TOKENS, 8), jnp.float32, -1.2, 1.2)
    factors = jnp.repeat(jnp.exp(logs), D // 8, axis=1)
    return (base * factors).astype(jnp.bfloat16)


def draw_decay_rate(key, part):
    picks = jax.random.randint(jax.random.fold_in(key, 21), (HEADS,), 0, 2)
    quick = jax.random.uniform(jax.random.fold_in(key, 22), (HEADS,), jnp.float32, 4.0 / BLK, 16.0 / BLK)
    slower = jax.random.uniform(jax.random.fold_in(key, 23), (HEADS,), jnp.float32, 0.3 / LEN, 2.3 / LEN)
    return jnp.where(picks == 1, quick, slower)


def steps_of(rng, extent, split, low, high):
    factor_of, own = 1.0, jax.random.fold_in(rng, 6)
    for position, blocks in split:
        heights = jnp.exp(jax.random.uniform(jax.random.fold_in(own, position), (blocks,), jnp.float32, low / len(split), high / len(split)))
        factor_of = factor_of * jnp.repeat(heights, extent[position] // blocks).reshape([-1 if axis == position else 1 for axis in range(len(extent))])
    return factor_of


def centred(rng, dims, deviation, most, split=(), held_as=jnp.bfloat16):
    array = deviation * jax.random.normal(rng, dims, jnp.float32)
    if split:
        array = array * steps_of(rng, dims, split, -0.22, 0.18)
    return jnp.clip(array, -most, most).astype(held_as)


def setup_inputs(seed: int = 0) -> dict:
    seeds = jax.random.split(jax.random.key(seed), 23)
    tokens = draw_tokens(jax.random.fold_in(seeds[22], 71), 0)
    gain_one = jnp.clip(1.0 + 0.18 * jax.random.normal(seeds[1], (D,), jnp.float32), 0.1, 1.9)
    w_gate = centred(seeds[2], (D, FF), D ** -0.5, 0.125, ((0, 16), (1, 8)), jnp.float32)
    w_up = centred(seeds[3], (D, FF), D ** -0.5, 0.125, ((0, 16), (1, 8)), jnp.float32)
    w_down = centred(seeds[4], (FF, D), FF ** -0.5, 0.109375, ((0, 8), (1, 16)), jnp.float32)
    scale_gate = jnp.clip(jnp.exp(math.log(2.0) - 1.3862944 * jax.random.uniform(seeds[5], (FF,), jnp.float32) ** steps_of(seeds[5], (FF,), ((0, 8),), -0.2, 0.2)), 0.5, 2.0)
    scale_up = jnp.clip(jnp.exp(math.log(2.0) - 1.3862944 * jax.random.uniform(seeds[6], (FF,), jnp.float32) ** steps_of(seeds[6], (FF,), ((0, 8),), -0.2, 0.2)), 0.5, 2.0)
    scale_down = jnp.clip(jnp.exp(math.log(2.0) - 1.3862944 * jax.random.uniform(seeds[7], (D,), jnp.float32) ** steps_of(seeds[7], (D,), ((0, 8),), -0.2, 0.2)), 0.5, 2.0)
    gain_mix = jnp.clip(1.0 + 0.18 * jax.random.normal(seeds[8], (D,), jnp.float32), 0.1, 1.9)
    w_query = centred(seeds[9], (D, RW), D ** -0.5, 0.125, ((0, 16), (1, 8)), jnp.float32)
    w_key = centred(seeds[10], (D, RW), D ** -0.5, 0.125, ((0, 16), (1, 8)), jnp.float32)
    w_value = centred(seeds[11], (D, RW), D ** -0.5, 0.125, ((0, 16), (1, 8)), jnp.float32)
    w_outgate = centred(seeds[12], (D, RW), D ** -0.5, 0.125, ((0, 16), (1, 8)), jnp.float32)
    scale_query = jnp.clip(jnp.exp(math.log(2.0) - 1.3862944 * jax.random.uniform(seeds[13], (RW,), jnp.float32) ** steps_of(seeds[13], (RW,), ((0, 8),), -0.2, 0.2)), 0.5, 2.0)
    scale_key = jnp.clip(jnp.exp(math.log(2.0) - 1.3862944 * jax.random.uniform(seeds[14], (RW,), jnp.float32) ** steps_of(seeds[14], (RW,), ((0, 8),), -0.2, 0.2)), 0.5, 2.0)
    scale_value = jnp.clip(jnp.exp(math.log(2.0) - 1.3862944 * jax.random.uniform(seeds[15], (RW,), jnp.float32) ** steps_of(seeds[15], (RW,), ((0, 8),), -0.2, 0.2)), 0.5, 2.0)
    scale_outgate = jnp.clip(jnp.exp(math.log(2.0) - 1.3862944 * jax.random.uniform(seeds[16], (RW,), jnp.float32) ** steps_of(seeds[16], (RW,), ((0, 8),), -0.2, 0.2)), 0.5, 2.0)
    ret_gain = jnp.clip(1.0 + 0.18 * jax.random.normal(seeds[17], (RW,), jnp.float32), 0.1, 1.9)
    decay_rate = draw_decay_rate(jax.random.fold_in(seeds[22], 71), 0)
    w_mix = centred(seeds[19], (RW, D), RW ** -0.5, 0.125, ((0, 8), (1, 16)), jnp.float32)
    scale_mix = jnp.clip(jnp.exp(math.log(2.0) - 1.3862944 * jax.random.uniform(seeds[20], (D,), jnp.float32) ** steps_of(seeds[20], (D,), ((0, 8),), -0.2, 0.2)), 0.5, 2.0)
    gain_two = jnp.clip(1.0 + 0.18 * jax.random.normal(seeds[21], (D,), jnp.float32), 0.1, 1.9)
    return dict(tokens=tokens, gain_one=gain_one, w_gate=w_gate, w_up=w_up, w_down=w_down, scale_gate=scale_gate, scale_up=scale_up, scale_down=scale_down, gain_mix=gain_mix, w_query=w_query, w_key=w_key, w_value=w_value, w_outgate=w_outgate, scale_query=scale_query, scale_key=scale_key, scale_value=scale_value, scale_outgate=scale_outgate, ret_gain=ret_gain, decay_rate=decay_rate, w_mix=w_mix, scale_mix=scale_mix, gain_two=gain_two)


EPS = 1e-06
HEAD_EPS = 0.1

def rms_rows(hidden_in, norm_gain):
    widened = hidden_in.astype(jnp.float32)
    scaled = widened * lax.rsqrt(lax.optimization_barrier(jnp.mean(widened * widened, axis=1, keepdims=True)) + EPS) * norm_gain
    return scaled.astype(jnp.bfloat16)

def project(features, weight, column_scale):
    return jnp.dot(features, weight.astype(jnp.bfloat16), preferred_element_type=jnp.float32) * column_scale

def split_sum(left, weight, parts):
    width = left.shape[1] // parts

    def add_block(index, total):
        start = (index * width).astype(jnp.int32)
        columns = lax.dynamic_slice_in_dim(left, start, width, 1)
        block = lax.dynamic_slice_in_dim(weight, start, width, 0).astype(jnp.bfloat16)
        partial_value = jnp.dot(columns, block, preferred_element_type=jnp.float32).astype(jnp.bfloat16)
        partial_value = lax.optimization_barrier(partial_value)
        return total + partial_value.astype(jnp.float32)
    return lax.fori_loop(0, parts, add_block, jnp.zeros((left.shape[0], weight.shape[1]), jnp.float32))

def feed_forward(features, w_gate, w_up, w_down, scale_gate, scale_up, scale_down):
    gate_pre = project(features, w_gate, scale_gate)
    up_pre = project(features, w_up, scale_up)
    hidden = (jax.nn.silu(gate_pre) * up_pre).astype(jnp.bfloat16)
    return split_sum(hidden, w_down, N_TP) * scale_down

def rotate_pairs(values):
    paired = values.reshape(values.shape[:-1] + (values.shape[-1] // 2, 2))
    return jnp.stack((-paired[..., 1], paired[..., 0]), axis=-1).reshape(values.shape)

def retain(query_rows, key_rows, value_rows, decay_rate, length, block):
    highest = lax.Precision.HIGHEST
    total_rows = query_rows.shape[0]
    heads = decay_rate.shape[0]
    head_size = query_rows.shape[1] // heads
    sequences = total_rows // length
    nblocks = length // block

    def split_heads(values):
        return values.astype(jnp.float32).reshape(sequences, length, heads, head_size)
    freq = 1.0 / 10000.0 ** jnp.linspace(0.0, 1.0, head_size // 2, dtype=jnp.float32)
    freq = jnp.repeat(freq, 2)
    angles = jnp.arange(length, dtype=jnp.float32)[:, None] * freq[None, :]
    sines = jnp.sin(angles)[None, :, None, :]
    cosines = jnp.cos(angles)[None, :, None, :]
    queries = split_heads(query_rows)
    queries = queries * cosines + rotate_pairs(queries) * sines
    keys_all = split_heads(key_rows) * head_size ** (-0.5)
    keys_all = keys_all * cosines + rotate_pairs(keys_all) * sines
    values_all = split_heads(value_rows)
    log_decay = -decay_rate.astype(jnp.float32)
    offsets = jnp.arange(block, dtype=jnp.float32)
    distance = offsets[:, None] - offsets[None, :]
    inside = jnp.where(distance >= 0, jnp.exp(log_decay[:, None, None] * jnp.maximum(distance, 0.0)), 0.0)
    query_decay = jnp.exp(log_decay[None, :] * (offsets[:, None] + 1.0))
    key_decay = jnp.exp(log_decay[None, :] * (block - 1.0 - offsets[:, None]))
    block_decay = jnp.exp(log_decay * block)

    def to_blocks(values):
        return jnp.moveaxis(values.reshape(sequences, nblocks, block, heads, head_size), 1, 0)

    def advance(carried, pieces):
        query_blk, key_blk, value_blk = pieces
        scores = jnp.einsum('snhd,smhd->shnm', query_blk, key_blk, precision=highest) * inside
        within = jnp.einsum('shnm,smhe->snhe', scores, value_blk, precision=highest)
        across = jnp.einsum('snhd,shde->snhe', query_blk, carried, precision=highest) * query_decay[None, :, :, None]
        weighted = key_blk * key_decay[None, :, :, None]
        carried = carried * block_decay[None, :, None, None] + jnp.einsum('smhd,smhe->shde', weighted, value_blk, precision=highest)
        return (carried, within + across)
    initial = jnp.zeros((sequences, heads, head_size, head_size), jnp.float32)
    _, results = lax.scan(advance, initial, (to_blocks(queries), to_blocks(keys_all), to_blocks(values_all)))
    results = jnp.moveaxis(results, 0, 1).reshape(sequences, length, heads, head_size)
    results = results * lax.rsqrt(lax.optimization_barrier(jnp.mean(results * results, axis=-1, keepdims=True)) + HEAD_EPS)
    return results.reshape(total_rows, heads * head_size)

def reference(tokens, gain_one, w_gate, w_up, w_down, scale_gate, scale_up, scale_down, gain_mix, w_query, w_key, w_value, w_outgate, scale_query, scale_key, scale_value, scale_outgate, ret_gain, decay_rate, w_mix, scale_mix, gain_two):
    ffn_one = feed_forward(rms_rows(tokens, gain_one), w_gate, w_up, w_down, scale_gate, scale_up, scale_down)
    first = (tokens.astype(jnp.float32) + 0.5 * ffn_one).astype(jnp.bfloat16)
    features = rms_rows(first, gain_mix)
    query_rows = project(features, w_query, scale_query).astype(jnp.bfloat16)
    key_rows = project(features, w_key, scale_key).astype(jnp.bfloat16)
    value_rows = project(features, w_value, scale_value).astype(jnp.bfloat16)
    outgate_rows = project(features, w_outgate, scale_outgate).astype(jnp.bfloat16)
    retained = retain(query_rows, key_rows, value_rows, decay_rate, LEN, BLK)
    mixed = (retained * ret_gain * jax.nn.silu(outgate_rows.astype(jnp.float32))).astype(jnp.bfloat16)
    second = (first.astype(jnp.float32) + split_sum(mixed, w_mix, N_TP) * scale_mix).astype(jnp.bfloat16)
    ffn_two = feed_forward(rms_rows(second, gain_two), w_gate, w_up, w_down, scale_gate, scale_up, scale_down)
    return (second.astype(jnp.float32) + 0.5 * ffn_two).astype(jnp.bfloat16)
```

```python
import functools

import jax
import jax.numpy as jnp
import numpy as np
from jax import lax
from jax.experimental import pallas as pl
from jax.experimental.pallas import tpu as pltpu
from jax.sharding import PartitionSpec as P

MESH = pl.DeviceIdType.MESH
BF16 = jnp.bfloat16
F32 = jnp.float32

D = 2048
LEN = 256
ROWS = 256
CHUNKS = 3
EPS = 1e-06
HEAD_EPS = 0.1
GROUPS = ("gu", "dn", "qk", "mx")
PIECE_ROWS = {"gu": 128, "dn": 384, "qk": 128, "mx": 256}
PIECE_BYTES = {"gu": 196608, "dn": 98304, "qk": 262144, "mx": 65536}
BLOCK = 131072


class Step:
    def __init__(self, run, waits=(), sends=(), needs=(), gives=None, cost=0.1, rank=1.0):
        self.run, self.waits, self.sends = run, waits, sends
        self.needs, self.gives, self.cost, self.rank = needs, gives, cost, rank


def link_time(way, size):
    return size / (300e3 if way == "d" else 45e3)


def in_order(lists):
    clock, arrive, free, given, order = 3.0, {}, {}, set(), []
    for key, when in (("hbm", 3.5),):
        arrive[key] = when
    heads = [0] * len(lists)
    while True:
        best = None
        for number, steps in enumerate(lists):
            if heads[number] == len(steps):
                continue
            step = steps[heads[number]]
            if any(k not in given for k in step.needs) or any(k not in arrive for k in step.waits):
                continue
            ready = max([clock] + [arrive[k] for k in step.waits])
            score = (ready, step.rank, number)
            if best is None or score < best[0]:
                best = (score, number, step)
        if best is None:
            break
        (ready, _, _), number, step = best
        heads[number] += 1
        clock = ready + step.cost
        for way, size, key in step.sends:
            done = max(free.get(way, 0.0), clock) + link_time(way, size)
            free[way] = done
            arrive[key] = max(arrive.get(key, 0.0), done + (1.0 if way == "d" else 2.2))
        if step.gives is not None:
            given.add(step.gives)
        order.append((clock, step))
    assert all(h == len(s) for h, s in zip(heads, lists))
    return order


class Sems:
    def __init__(self, ref):
        self.ref, self.at = ref, {}

    def __getitem__(self, key):
        if key not in self.at:
            self.at[key] = len(self.at)
        return self.ref.at[self.at[key]]


NSEM_RECV = 192
NSEM_SEND = 24


def layer_kernel(
    tokens, w_gate, w_up, w_down, w_query, w_key, w_value, w_outgate, w_mix, cos_t, sin_t,
    gain_one, gain_mix, gain_two, s_gate, s_up, s_down, s_query, s_key, s_value, s_outgate,
    ret_gain, decay, s_mix,
    out,
    W_gu, W_dn, W_qk, W_mx,
    F_gu, F_dn, F_qk, F_mx,
    COS, SIN, DEC, GB, XG, NX, HID, QB, MX, OB, PB, RD, SB, R1, FIN, OUT,
    hbm_sem, recv_sem, send_sem,
):
    fs, tp = lax.axis_index("fs"), lax.axis_index("tp")
    z, y = fs // 4, fs % 4
    x, c = tp // 2, tp % 2

    def around(v, k):
        return (v + k) % 4

    def fs_of(zz, yy):
        return zz * 4 + yy

    def tp_of(k, core):
        return around(x, k) * 2 + core

    where = {
        "x+": (fs, tp_of(1, c)), "x-": (fs, tp_of(3, c)), "d": (fs, x * 2 + (1 - c)),
        "y+": (fs_of(z, around(y, 1)), tp), "y-": (fs_of(z, around(y, 3)), tp),
        "z+": (fs_of(around(z, 1), y), tp), "z-": (fs_of(around(z, 3), y), tp),
    }
    W = {"gu": W_gu, "dn": W_dn, "qk": W_qk, "mx": W_mx}
    recv, sent = Sems(recv_sem), Sems(send_sem)

    def copy(src, dst, send_key, recv_key, way):
        return pltpu.make_async_remote_copy(
            src_ref=src, dst_ref=dst, send_sem=sent[send_key], recv_sem=recv[recv_key],
            device_id=where[way], device_id_type=MESH,
        )

    def send(ref, send_key, recv_key, way, dst=None):
        copy(ref, ref if dst is None else dst, send_key, recv_key, way).start()

    def got(ref, send_key, recv_key):
        copy(ref, ref, send_key, recv_key, "d").wait_recv()

    def left(ref, send_key, recv_key):
        copy(ref, ref, send_key, recv_key, "d").wait_send()

    loads = {}

    def load(key, src, dst):
        loads[key] = pltpu.make_async_copy(src, dst, hbm_sem.at[len(loads)])
        loads[key].start()

    load("g", w_gate, F_gu.at[0])
    load("u", w_up, F_gu.at[1])
    for k in range(CHUNKS):
        load(("t", k), tokens.at[pl.ds(k * ROWS, ROWS), :], XG.at[k, tp])
    load("d", w_down, F_dn)
    for n, w in enumerate((w_query, w_key, w_value, w_outgate)):
        load(("q", n), w, F_qk.at[n])
    load("m", w_mix, F_mx)
    load("cos", cos_t, COS)
    load("sin", sin_t, SIN)

    barrier = pltpu.get_barrier_semaphore()
    for way in ("x+", "x-", "d", "y+", "y-", "z+", "z-"):
        pl.semaphore_signal(barrier, inc=1, device_id=where[way], device_id_type=MESH)

    lists = []

    def wpart(g, f, half, quarter=None):
        n = PIECE_ROWS[g] // 2
        lo = n * half
        if quarter is not None:
            n //= 2
            lo += n * quarter
        if g in ("gu", "qk"):
            return W[g].at[pl.ds(pl.multiple_of(f * 128 + lo, 32), n), :]
        return W[g].at[pl.ds(lo, n), pl.ds(pl.multiple_of(f * 128, 128), 128)]

    def wspan(g, pieces):
        if g in ("gu", "qk"):
            return W[g].at[pl.ds(0, 128 * pieces), :]
        return W[g].at[:, pl.ds(0, 128 * pieces)]

    def cast_gu():
        loads["g"].wait()
        loads["u"].wait()
        rows = pl.ds(pl.multiple_of(fs * 128, 128), 128)
        for j in range(3):
            W_gu[rows, 256 * j : 256 * j + 128] = F_gu[0, :, 128 * j : 128 * j + 128].astype(BF16)
            W_gu[rows, 256 * j + 128 : 256 * j + 256] = F_gu[1, :, 128 * j : 128 * j + 128].astype(BF16)

    def cast_dn():
        loads["d"].wait()
        W_dn[:, pl.ds(pl.multiple_of(fs * 128, 128), 128)] = F_dn[...].astype(BF16)

    def cast_qk():
        rows = pl.ds(pl.multiple_of(fs * 128, 128), 128)
        for n in range(4):
            loads[("q", n)].wait()
            W_qk[rows, 256 * n : 256 * n + 256] = F_qk[n].astype(BF16)

    def cast_mx():
        loads["m"].wait()
        W_mx[:, pl.ds(pl.multiple_of(fs * 128, 128), 128)] = F_mx[...].astype(BF16)

    casts = {"gu": cast_gu, "dn": cast_dn, "qk": cast_qk, "mx": cast_mx}
    cast_steps = []
    for n, g in enumerate(GROUPS):
        cast_steps.append(Step(casts[g], waits=("hbm",), gives=("cast", g), cost=0.3, rank=-5 if n == 0 else 1.5))
    lists.append(cast_steps)

    def weight_lists(order, g):
        rank = 0.2 + 0.1 * order
        for half in (0, 1):
            a, b = ("y", "z") if half == 0 else ("z", "y")

            def at(i, j, a=a):
                return fs_of(around(z, j), around(y, i)) if a == "y" else fs_of(around(z, i), around(y, j))

            full = PIECE_BYTES[g] // 2
            key = lambda *k, half=half: ("w", g, half) + k
            skey = ("w", g)

            def both(i, half=half, at=at, a=a, b=b, key=key, full=full):
                def run():
                    for way in (b + "+", b + "-"):
                        send(wpart(g, at(i, 0), half), skey, key("s", i, way[1]), way)
                return run, [(way, full, key("s", i, way[1])) for way in (b + "+", b + "-")]

            def own(half=half, at=at, a=a, b=b, key=key, full=full):
                more, extra = both(0)
                def run():
                    for way in (a + "+", a + "-"):
                        send(wpart(g, at(0, 0), half), skey, key("f", way[1]), way)
                    more()
                return run, [(way, full, key("f", way[1])) for way in (a + "+", a + "-")] + extra

            def first(side, half=half, at=at, a=a, b=b, key=key, full=full):
                i, back, q = (3, "+", 0) if side == "+" else (1, "-", 1)
                more, extra = both(i)
                def run():
                    got(wpart(g, at(i, 0), half), skey, key("f", side))
                    send(wpart(g, at(i, 0), half, q), skey, key("f2"), a + back)
                    more()
                return run, [(a + back, full // 2, key("f2"))] + extra

            def far(half=half, at=at, a=a, b=b, key=key):
                more, extra = both(2)
                def run():
                    got(wpart(g, at(2, 0), half), skey, key("f2"))
                    more()
                return run, extra

            def second(i, side, half=half, at=at, a=a, b=b, key=key, full=full):
                j, back, q = (3, "+", 0) if side == "+" else (1, "-", 1)
                def run():
                    got(wpart(g, at(i, j), half), skey, key("s", i, side))
                    send(wpart(g, at(i, j), half, q), skey, ("w", g, "end"), b + back)
                return run, [(b + back, full // 2, ("w", g, "end"))]

            run, sends = own()
            needs = [("cast", g)]
            if order:
                needs += [("far", GROUPS[order - 1], 0), ("far", GROUPS[order - 1], 1)]
            steps = [Step(run, sends=sends, needs=needs, gives=("own", g, half), rank=rank, cost=0.1)]
            for side in ("+", "-"):
                run, sends = first(side)
                steps.append(Step(run, waits=(key("f", side),), sends=sends, rank=rank))
            run, sends = far()
            steps.append(Step(run, waits=(key("f2"),), sends=sends, rank=rank, gives=("far", g, half)))
            lists.append(steps)
            steps = []
            for i in (0, 3, 1, 2):
                for side in ("+", "-"):
                    run, sends = second(i, side)
                    steps.append(Step(run, waits=(key("s", i, side),), sends=sends, rank=rank))
            steps[-1].gives = ("last", g, half)
            lists.append(steps)

        def end():
            got(wspan(g, 4), ("w", g), ("w", g, "end"))
        lists.append([Step(end, waits=(("w", g, "end"),), needs=(("last", g, 0), ("last", g, 1)), gives=("W", g), rank=rank)])

    for order, g in enumerate(GROUPS):
        weight_lists(order, g)

    def tables():
        loads["cos"].wait()
        loads["sin"].wait()
        n = lax.broadcasted_iota(jnp.int32, (LEN, LEN), 0)
        m = lax.broadcasted_iota(jnp.int32, (LEN, LEN), 1)
        distance = jnp.maximum(n - m, 0).astype(F32)
        DEC[...] = jnp.where(n >= m, jnp.exp(-decay[...] * distance), 0.0) * (LEN ** -0.5)

    lists.append([Step(tables, waits=("hbm",), gives="tables", rank=3.0, cost=0.3)])

    def chunk_list(k):
        steps = []
        base = 0.0 + 0.01 * k

        for s in range(3):
            n = s * CHUNKS + k
            xg = XG.at[n]
            akey, rkey = ("a", n), ("r", n)

            def slot(t, n=n):
                return XG.at[n, t]

            def half_of(t, h, n=n):
                return XG.at[n, t, pl.ds(128 * h, 128), :]

            gains = s == 0 and k == 0

            def a0(s=s, akey=akey, slot=slot, gains=gains):
                if s == 0:
                    loads[("t", k)].wait()
                for way, r in (("x+", "L"), ("x-", "R"), ("d", "D")):
                    send(slot(tp), akey, akey + (r,), way)
                if gains:
                    for i, gain in enumerate((gain_one, gain_mix, gain_two)):
                        GB[tp, i : i + 1, :] = gain[...]
                    for way, r in (("x+", "L"), ("x-", "R"), ("d", "D")):
                        send(GB.at[tp], ("g",), ("g", r), way)

            def a1(akey=akey, slot=slot, half_of=half_of, gains=gains):
                t = tp_of(3, c)
                got(slot(t), akey, akey + ("L",))
                send(half_of(t, 0), akey, akey + ("F",), "x+")
                send(slot(t), akey, akey + ("D",), "d")
                if gains:
                    got(GB.at[t], ("g",), ("g", "L"))
                    send(GB.at[t], ("g",), ("g", "F"), "x+")
                    send(GB.at[t], ("g",), ("g", "D"), "d")

            def a2(akey=akey, slot=slot, half_of=half_of, gains=gains):
                t = tp_of(1, c)
                got(slot(t), akey, akey + ("R",))
                send(half_of(t, 1), akey, akey + ("F",), "x-")
                send(slot(t), akey, akey + ("D",), "d")
                if gains:
                    got(GB.at[t], ("g",), ("g", "R"))
                    send(GB.at[t], ("g",), ("g", "D"), "d")

            def a3(akey=akey, slot=slot, gains=gains):
                t = tp_of(2, c)
                got(slot(t), akey, akey + ("F",))
                send(slot(t), akey, akey + ("D",), "d")
                if gains:
                    got(GB.at[t], ("g",), ("g", "F"))
                    send(GB.at[t], ("g",), ("g", "D"), "d")

            def normed(n=n, s=s, akey=akey, gains=gains):
                got(XG.at[n, pl.ds(0, 4)], akey, akey + ("D",))
                if gains:
                    got(GB.at[pl.ds(0, 4)], ("g",), ("g", "D"))

                def rows_of(i, carry):
                    r = pl.ds(pl.multiple_of(i * 16, 16), 16)
                    hs = [XG[n, t, r, :].astype(F32) for t in range(8)]
                    squares = hs[0] * hs[0]
                    for h in hs[1:]:
                        squares += h * h
                    scale = lax.rsqrt(jnp.sum(squares, axis=1, keepdims=True) / D + EPS)
                    for t in range(8):
                        NX[r, 256 * t : 256 * t + 256] = (hs[t] * scale * GB[t, s : s + 1, :]).astype(BF16)
                    return carry

                lax.fori_loop(0, ROWS // 16, rows_of, 0)

            def gate_up(normed=normed):
                normed()

                def cols_of(j, carry):
                    both = jnp.dot(
                        NX[...], W_gu[:, pl.ds(pl.multiple_of(j * 256, 256), 256)], preferred_element_type=F32
                    )
                    lane = pl.ds(pl.multiple_of(j * 128, 128), 128)
                    gate, up = both[:, :128] * s_gate[:, lane], both[:, 128:] * s_up[:, lane]
                    HID[k, :, lane] = (gate / (1.0 + jnp.exp(-gate)) * up).astype(BF16)
                    return carry

                lax.fori_loop(0, 3, cols_of, 0)

            def query_key(normed=normed):
                normed()
                for j, scale in enumerate((s_query, s_key, s_value, s_outgate)):
                    pre = jnp.dot(NX[...], W_qk[:, 256 * j : 256 * j + 256], preferred_element_type=F32)
                    QB[j] = (pre * scale[...]).astype(BF16)

            def turned(j):
                v = QB[j].astype(F32)
                even = lax.broadcasted_iota(jnp.int32, (LEN, 256), 1) % 2 == 0
                swapped = jnp.where(even, -pltpu.roll(v, 255, 1), pltpu.roll(v, 1, 1))
                return (v * COS[...] + swapped * SIN[...]).astype(BF16)

            def retained():
                scores = lax.dot_general(
                    turned(0), turned(1), (((1,), (1,)), ((), ())), preferred_element_type=F32
                )
                kept = jnp.dot((scores * DEC[...]).astype(BF16), QB[2], preferred_element_type=F32)
                kept = kept * lax.rsqrt(jnp.mean(kept * kept, axis=1, keepdims=True) + HEAD_EPS)
                gate = QB[3].astype(F32)
                MX[...] = (kept * ret_gain[...] * (gate / (1.0 + jnp.exp(-gate)))).astype(BF16)

            def product(i, core, s=s):
                cols = pl.ds(pl.multiple_of((around(x, i) * 2 + core) * 256, 256), 256)
                if s == 1:
                    return jnp.dot(MX[...], W_mx[:, cols], preferred_element_type=F32)
                return jnp.dot(HID[k], W_dn[:, cols], preferred_element_type=F32)

            def theirs(n=n, rkey=rkey, product=product):
                def block_of(i, carry):
                    PB[n, i] = product(i, 1 - c).astype(BF16)
                    return carry

                lax.fori_loop(0, 4, block_of, 0)
                for i, r in ((2, "2"), (1, "13"), (3, "13"), (0, "0")):
                    send(PB.at[n, i], rkey, rkey + (r,), "d", RD.at[n, i])

            def mine(product=product):
                def block_of(i, carry):
                    OB[k, i] = product(i, c)
                    return carry

                lax.fori_loop(0, 4, block_of, 0)

            def r0(n=n, rkey=rkey):
                got(RD.at[n, 2], rkey, rkey + ("2",))
                SB[n, 0] = (OB[k, 2] + RD[n, 2].astype(F32)).astype(BF16)
                send(SB.at[n, 0, pl.ds(0, 128)], rkey, rkey + ("L",), "x+", R1.at[n, 0])
                send(SB.at[n, 0, pl.ds(128, 128)], rkey, rkey + ("R",), "x-", R1.at[n, 1])

            def r1(n=n, rkey=rkey):
                got(RD.at[n, pl.ds(0, 2)], rkey, rkey + ("13",))
                upper = OB[k, 1, 128:256] + RD[n, 1, 128:256].astype(F32)
                SB[n, 1, 128:256] = upper.astype(BF16)
                send(SB.at[n, 1, pl.ds(128, 128)], rkey, rkey + ("E",), "x+", FIN.at[n, 0, pl.ds(128, 128)])
                lower = OB[k, 3, 0:128] + RD[n, 3, 0:128].astype(F32)
                SB[n, 2, 0:128] = lower.astype(BF16)
                send(SB.at[n, 2, pl.ds(0, 128)], rkey, rkey + ("E",), "x-", FIN.at[n, 1, pl.ds(0, 128)])

            def r2(n=n, rkey=rkey):
                got(R1.at[n, 0], rkey, rkey + ("L",))
                SB[n, 1, 0:128] = (
                    OB[k, 1, 0:128] + RD[n, 1, 0:128].astype(F32) + R1[n, 0].astype(F32)
                ).astype(BF16)
                send(SB.at[n, 1, pl.ds(0, 128)], rkey, rkey + ("E",), "x+", FIN.at[n, 0, pl.ds(0, 128)])

            def r3(n=n, rkey=rkey):
                got(R1.at[n, 1], rkey, rkey + ("R",))
                SB[n, 2, 128:256] = (
                    OB[k, 3, 128:256] + RD[n, 3, 128:256].astype(F32) + R1[n, 1].astype(F32)
                ).astype(BF16)
                send(SB.at[n, 2, pl.ds(128, 128)], rkey, rkey + ("E",), "x-", FIN.at[n, 1, pl.ds(128, 128)])

            def r4(n=n, s=s, rkey=rkey):
                got(RD.at[n, 0], rkey, rkey + ("0",))
                got(FIN.at[n], rkey, rkey + ("E",))
                total = OB[k, 0] + RD[n, 0].astype(F32) + FIN[n, 0].astype(F32) + FIN[n, 1].astype(F32)
                if s == 1:
                    total = total * s_mix[...]
                else:
                    total = 0.5 * total * s_down[...]
                after = (XG[n, tp].astype(F32) + total).astype(BF16)
                if s < 2:
                    XG[n + CHUNKS, tp] = after
                else:
                    OUT[k] = after
                    pltpu.make_async_copy(OUT.at[k], out.at[pl.ds(k * ROWS, ROWS), :], hbm_sem.at[20 + k]).start()

            L, R, F, Dk = (akey + (r,) for r in "LRFD")
            extra = (("g", "L"), ("g", "R"), ("g", "F"), ("g", "D"))
            sends = [("x+", BLOCK, L), ("x-", BLOCK, R), ("d", BLOCK, Dk)]
            waits = ("hbm",) if s == 0 else ()
            gsize = 8192
            add = lambda *pairs: [(w, gsize, q) for w, q in pairs] if gains else []
            more = lambda q: (q,) if gains else ()
            a0_step = Step(a0, waits=waits, sends=sends + add(("x+", extra[0]), ("x-", extra[1]), ("d", extra[3])),
                           rank=base + (0.0 if s else -1 + 0.1 * k), cost=0.1)
            steps.append(a0_step)
            steps.append(Step(a1, waits=(L,) + more(extra[0]),
                              sends=[("x+", BLOCK // 2, F), ("d", BLOCK, Dk)] + add(("x+", extra[2]), ("d", extra[3])), rank=base))
            steps.append(Step(a2, waits=(R,) + more(extra[1]),
                              sends=[("x-", BLOCK // 2, F), ("d", BLOCK, Dk)] + add(("d", extra[3])), rank=base))
            steps.append(Step(a3, waits=(F,) + more(extra[2]), sends=[("d", BLOCK, Dk)] + add(("d", extra[3])), rank=base))
            if s == 1:
                steps.append(Step(query_key, waits=(Dk,), needs=(("W", "qk"),), rank=2 + base, cost=2.0))
                steps.append(Step(retained, needs=("tables",), rank=2 + base, cost=0.7))
                end = ("W", "mx")
            else:
                needs = (("W", "gu"),) if gains else (("W", "gu"), "gains")
                steps.append(Step(gate_up, waits=(Dk,) + more(extra[3]), needs=needs, rank=2 + base, cost=1.8,
                                  gives="gains" if gains else None))
                end = ("W", "dn")
            r = lambda q: rkey + (q,)
            steps.append(Step(theirs, needs=(end,), rank=2 + base, cost=0.5,
                              sends=[("d", BLOCK, r("2")), ("d", BLOCK, r("13")), ("d", BLOCK, r("13")), ("d", BLOCK, r("0"))]))
            steps.append(Step(mine, rank=2 + base, cost=0.5))
            steps.append(Step(r0, waits=(r("2"),), rank=base, sends=[("x+", BLOCK // 2, r("L")), ("x-", BLOCK // 2, r("R"))], cost=0.15))
            steps.append(Step(r1, waits=(r("13"),), rank=base, sends=[("x+", BLOCK // 2, r("E")), ("x-", BLOCK // 2, r("E"))], cost=0.15))
            steps.append(Step(r2, waits=(r("L"),), rank=base, sends=[("x+", BLOCK // 2, r("E"))]))
            steps.append(Step(r3, waits=(r("R"),), rank=base, sends=[("x-", BLOCK // 2, r("E"))]))
            steps.append(Step(r4, waits=(r("E"), r("0")), rank=base, cost=0.2))
        return steps

    for k in range(CHUNKS):
        lists.append(chunk_list(k))

    order = in_order(lists)
    pl.semaphore_wait(barrier, 7)
    for _, step in order:
        step.run()

    for g in GROUPS:
        left(wspan(g, 15), ("w", g), ("w", g, "end"))
    left(GB.at[pl.ds(0, 7)], ("g",), ("g", "D"))
    for n in range(3 * CHUNKS):
        left(XG.at[n, pl.ds(0, 7)], ("a", n), ("a", n, "D"))
        left(XG.at[n, pl.ds(0, 7)], ("r", n), ("r", n, "0"))
    for k in range(CHUNKS):
        pltpu.make_async_copy(OUT.at[k], out.at[pl.ds(k * ROWS, ROWS), :], hbm_sem.at[20 + k]).wait()
    assert len(recv.at) <= NSEM_RECV and len(sent.at) <= NSEM_SEND


def per_device(
    tokens, gain_one, w_gate, w_up, w_down, scale_gate, scale_up, scale_down, gain_mix,
    w_query, w_key, w_value, w_outgate, scale_query, scale_key, scale_value, scale_outgate,
    ret_gain, decay_rate, w_mix, scale_mix, gain_two,
):
    freq = (1.0 / 10000.0 ** np.linspace(0.0, 1.0, 128)).astype(np.float32)
    angles = (np.arange(LEN, dtype=np.float32)[:, None] * np.repeat(freq, 2)[None, :]).astype(np.float64)
    cos_t = jnp.asarray(np.cos(angles), F32)
    sin_t = jnp.asarray(np.sin(angles), F32)
    row = lambda v: v.reshape(1, -1)
    small = [row(v) for v in (
        gain_one, gain_mix, gain_two, scale_gate, scale_up, scale_down, scale_query, scale_key, scale_value,
        scale_outgate, ret_gain, decay_rate, scale_mix,
    )]
    anywhere = pl.BlockSpec(memory_space=pl.ANY)
    vmem = pl.BlockSpec(memory_space=pltpu.VMEM)
    V = pltpu.VMEM
    nine = 3 * CHUNKS
    return pl.pallas_call(
        layer_kernel,
        out_shape=jax.ShapeDtypeStruct((CHUNKS * ROWS, 256), BF16),
        in_specs=[anywhere] * 11 + [vmem] * len(small),
        out_specs=anywhere,
        scratch_shapes=[
            V((2048, 768), BF16), V((384, 2048), BF16), V((2048, 1024), BF16), V((256, 2048), BF16),
            V((2, 128, 384), F32), V((384, 128), F32), V((4, 128, 256), F32), V((256, 128), F32),
            V((LEN, 256), F32), V((LEN, 256), F32), V((LEN, LEN), F32), V((8, 8, 256), F32),
            V((nine, 8, ROWS, 256), BF16), V((ROWS, D), BF16), V((CHUNKS, ROWS, 384), BF16),
            V((4, ROWS, 256), BF16), V((ROWS, 256), BF16), V((CHUNKS, 4, ROWS, 256), F32),
            V((nine, 4, ROWS, 256), BF16), V((nine, 4, ROWS, 256), BF16), V((nine, 3, ROWS, 256), BF16),
            V((nine, 2, 128, 256), BF16), V((nine, 2, ROWS, 256), BF16), V((CHUNKS, ROWS, 256), BF16),
            pltpu.SemaphoreType.DMA((24,)), pltpu.SemaphoreType.DMA((NSEM_RECV,)), pltpu.SemaphoreType.DMA((NSEM_SEND,)),
        ],
        compiler_params=pltpu.CompilerParams(
            collective_id=0, has_side_effects=True, vmem_limit_bytes=60 * 1024 * 1024
        ),
        name="layer",
    )(tokens, w_gate, w_up, w_down, w_query, w_key, w_value, w_outgate, w_mix, cos_t, sin_t, *small)


def solution(mesh):
    return jax.shard_map(
        per_device,
        mesh=mesh,
        in_specs=(
            P("fs", "tp"), P("tp"), P("fs", "tp"), P("fs", "tp"), P("tp", "fs"), P("tp"), P("tp"), P("tp"), P("tp"),
            P("fs", "tp"), P("fs", "tp"), P("fs", "tp"), P("fs", "tp"), P("tp"), P("tp"), P("tp"), P("tp"), P("tp"),
            P("tp"), P("tp", "fs"), P("tp"), P("tp"),
        ),
        out_specs=P("fs", "tp"),
        check_vma=False,
    )
```

```python
import functools

import jax
import jax.numpy as jnp
import numpy as np
from jax import lax
from jax.experimental import pallas as pl
from jax.experimental.pallas import tpu as pltpu
from jax.sharding import PartitionSpec as P

MESH = pl.DeviceIdType.MESH
BF16 = jnp.bfloat16
F32 = jnp.float32

D = 2048
LEN = 256
ROWS = 128
HALF = ROWS // 2
CHUNKS = 6
EPS = 1e-06
HEAD_EPS = 0.1
GROUPS = ("gu", "dn", "qk", "mx")
PIECE_ROWS = {"gu": 128, "dn": 384, "qk": 128, "mx": 256}
PIECE_BYTES = {"gu": 196608, "dn": 98304, "qk": 262144, "mx": 65536}
BLOCK = ROWS * 512


class Step:
    def __init__(self, run, waits=(), sends=(), needs=(), gives=None, cost=0.02, rank=1.0):
        self.run, self.waits, self.sends = run, waits, sends
        self.needs, self.gives, self.cost, self.rank = needs, gives, cost, rank


START = 1.5
MARGIN = 0.3
LATENCY = 2.6
WAYS = ("x+", "x-", "d", "y+", "y-", "z+", "z-")
GROUP_GAP = 2.5
STAGE_GAP = 10.0
COST = {"norm": 0.37, "gu": 0.73, "qk": 0.83, "ret": 0.4, "dn": 0.32, "mx": 0.25}
GATE = (None, None, None)


def link_time(way, size):
    return size / (300e3 if way == "d" else 45.7e3)


def in_order(lists):
    clock, free, given, order = 0.0, {}, set(), []
    arrive = {"hbm": 0.5}
    for way in WAYS:
        free[way] = START
    pending = {way: [] for way in WAYS}
    heads = [0] * len(lists)
    count = 0

    def issue(way, entry):
        _, _, size, key, step, which = entry
        done = max(free[way], clock) + link_time(way, size)
        free[way] = done
        arrive[key] = max(arrive.get(key, 0.0), done + (0.9 if way == "d" else LATENCY))
        missing[key] -= 1
        order.append((clock, step, which))

    missing = {"hbm": 0}
    for steps in lists:
        for step in steps:
            for _, _, key, _ in step.sends:
                missing[key] = missing.get(key, 0) + 1

    while True:
        best = None
        for number, steps in enumerate(lists):
            if heads[number] == len(steps):
                continue
            step = steps[heads[number]]
            if any(k not in given for k in step.needs) or any(missing[k] for k in step.waits):
                continue
            ready = max([clock] + [arrive[k] for k in step.waits])
            score = (ready, step.rank, number)
            if best is None or score < best[0]:
                best = (score, number, step)
        horizon = 1e9 if best is None else best[0][0] + best[2].cost + MARGIN
        issued = False
        for way in WAYS:
            if pending[way] and (way == "d" or free[way] < horizon):
                pending[way].sort(key=lambda e: e[:2])
                issue(way, pending[way].pop(0))
                issued = True
        if issued:
            continue
        if best is None:
            break
        (ready, _, _), number, step = best
        heads[number] += 1
        clock = ready + step.cost
        if step.gives is not None:
            given.add(step.gives)
        order.append((clock, step, None))
        for which, (way, size, key, urgency) in enumerate(step.sends):
            pending[way].append((urgency, count, size, key, step, which))
            count += 1
    assert all(h == len(s) for h, s in zip(heads, lists))
    return order


class Sems:
    def __init__(self, ref):
        self.ref, self.at = ref, {}

    def __getitem__(self, key):
        if key not in self.at:
            self.at[key] = len(self.at)
        return self.ref.at[self.at[key]]


NSEM_RECV = 288
NSEM_SEND = 48


def layer_kernel(
    tokens, w_gate, w_up, w_down, w_query, w_key, w_value, w_outgate, w_mix, cos_t, sin_t,
    gain_one, gain_mix, gain_two, s_gate, s_up, s_down, s_query, s_key, s_value, s_outgate,
    ret_gain, decay, s_mix,
    out,
    W_gu, W_dn, W_qk, W_mx,
    F_gu, F_dn, F_qk, F_mx,
    COS, SIN, DEC, GB, XG, NX, HID, QB, OG, KB, VB, MX, OB, PB, RD, SB, R1, FIN, OUT,
    hbm_sem, recv_sem, send_sem,
):
    fs, tp = lax.axis_index("fs"), lax.axis_index("tp")
    z, y = fs // 4, fs % 4
    x, c = tp // 2, tp % 2

    def around(v, k):
        return (v + k) % 4

    def fs_of(zz, yy):
        return zz * 4 + yy

    def tp_of(k, core):
        return around(x, k) * 2 + core

    where = {
        "x+": (fs, tp_of(1, c)), "x-": (fs, tp_of(3, c)), "d": (fs, x * 2 + (1 - c)),
        "y+": (fs_of(z, around(y, 1)), tp), "y-": (fs_of(z, around(y, 3)), tp),
        "z+": (fs_of(around(z, 1), y), tp), "z-": (fs_of(around(z, 3), y), tp),
    }
    W = {"gu": W_gu, "dn": W_dn, "qk": W_qk, "mx": W_mx}
    recv, sent = Sems(recv_sem), Sems(send_sem)

    def copy(src, dst, send_key, recv_key, way):
        return pltpu.make_async_remote_copy(
            src_ref=src, dst_ref=dst, send_sem=sent[send_key], recv_sem=recv[recv_key],
            device_id=where[way], device_id_type=MESH,
        )

    held = []

    def send(ref, send_key, recv_key, way, dst=None):
        held.append((way, lambda: copy(ref, ref if dst is None else dst, send_key, recv_key, way).start()))

    def got(ref, send_key, recv_key):
        copy(ref, ref, send_key, recv_key, "d").wait_recv()

    def left(ref, send_key, recv_key):
        copy(ref, ref, send_key, recv_key, "d").wait_send()

    loads = {}

    def load(key, src, dst):
        loads[key] = pltpu.make_async_copy(src, dst, hbm_sem.at[len(loads)])
        loads[key].start()

    load("g", w_gate, F_gu.at[0])
    load("u", w_up, F_gu.at[1])
    for k in range(CHUNKS):
        load(("t", k), tokens.at[pl.ds(k * ROWS, ROWS), :], XG.at[k, tp])
    load("d", w_down, F_dn)
    for n, w in enumerate((w_query, w_key, w_value, w_outgate)):
        load(("q", n), w, F_qk.at[n])
    load("m", w_mix, F_mx)
    load("cos", cos_t, COS)
    load("sin", sin_t, SIN)

    barrier = pltpu.get_barrier_semaphore()
    for way in WAYS:
        pl.semaphore_signal(barrier, inc=1, device_id=where[way], device_id_type=MESH)

    lists = []

    def wpart(g, f, half, quarter=None):
        n = PIECE_ROWS[g] // 2
        lo = n * half
        if quarter is not None:
            n //= 2
            lo += n * quarter
        if g in ("gu", "qk"):
            return W[g].at[pl.ds(pl.multiple_of(f * 128 + lo, 32), n), :]
        return W[g].at[pl.ds(lo, n), pl.ds(pl.multiple_of(f * 128, 128), 128)]

    def wspan(g, pieces):
        if g in ("gu", "qk"):
            return W[g].at[pl.ds(0, 128 * pieces), :]
        return W[g].at[:, pl.ds(0, 128 * pieces)]

    def cast_gu():
        loads["g"].wait()
        loads["u"].wait()
        rows = pl.ds(pl.multiple_of(fs * 128, 128), 128)
        for j in range(3):
            W_gu[rows, 256 * j : 256 * j + 128] = F_gu[0, :, 128 * j : 128 * j + 128].astype(BF16)
            W_gu[rows, 256 * j + 128 : 256 * j + 256] = F_gu[1, :, 128 * j : 128 * j + 128].astype(BF16)

    def cast_dn():
        loads["d"].wait()
        W_dn[:, pl.ds(pl.multiple_of(fs * 128, 128), 128)] = F_dn[...].astype(BF16)

    def cast_qk():
        rows = pl.ds(pl.multiple_of(fs * 128, 128), 128)
        for n in range(4):
            loads[("q", n)].wait()
            W_qk[rows, 256 * n : 256 * n + 256] = F_qk[n].astype(BF16)

    def cast_mx():
        loads["m"].wait()
        W_mx[:, pl.ds(pl.multiple_of(fs * 128, 128), 128)] = F_mx[...].astype(BF16)

    casts = {"gu": cast_gu, "dn": cast_dn, "qk": cast_qk, "mx": cast_mx}
    cast_steps = []
    for n, g in enumerate(GROUPS):
        cast_steps.append(Step(casts[g], waits=("hbm",), gives=("cast", g), cost=0.05, rank=-5 if n == 0 else 1.5))
    lists.append(cast_steps)

    def weight_lists(order, g):
        rank = 0.2 + 0.1 * order
        base = GROUP_GAP * order
        for half in (0, 1):
            a, b = ("y", "z") if half == 0 else ("z", "y")

            def at(i, j, a=a):
                return fs_of(around(z, j), around(y, i)) if a == "y" else fs_of(around(z, i), around(y, j))

            full = PIECE_BYTES[g] // 2
            key = lambda *k, half=half: ("w", g, half) + k
            skey = ("w", g)

            def both(i, half=half, at=at, a=a, b=b, key=key, full=full):
                def run():
                    for way in (b + "+", b + "-"):
                        send(wpart(g, at(i, 0), half), skey, key("s", i, way[1]), way)
                return run, [(way, full, key("s", i, way[1]), base + (2 if i else 1.5)) for way in (b + "+", b + "-")]

            def own(half=half, at=at, a=a, b=b, key=key, full=full):
                more, extra = both(0)
                def run():
                    for way in (a + "+", a + "-"):
                        send(wpart(g, at(0, 0), half), skey, key("f", way[1]), way)
                    more()
                return run, [(way, full, key("f", way[1]), base) for way in (a + "+", a + "-")] + extra

            def first(side, half=half, at=at, a=a, b=b, key=key, full=full):
                i, back, q = (3, "+", 0) if side == "+" else (1, "-", 1)
                more, extra = both(i)
                def run():
                    got(wpart(g, at(i, 0), half), skey, key("f", side))
                    send(wpart(g, at(i, 0), half, q), skey, key("f2"), a + back)
                    more()
                return run, [(a + back, full // 2, key("f2"), base + 1)] + extra

            def far(half=half, at=at, a=a, b=b, key=key):
                more, extra = both(2)
                def run():
                    got(wpart(g, at(2, 0), half), skey, key("f2"))
                    more()
                return run, extra

            def second(i, side, half=half, at=at, a=a, b=b, key=key, full=full):
                j, back, q = (3, "+", 0) if side == "+" else (1, "-", 1)
                def run():
                    got(wpart(g, at(i, j), half), skey, key("s", i, side))
                    send(wpart(g, at(i, j), half, q), skey, ("w", g, "end"), b + back)
                return run, [(b + back, full // 2, ("w", g, "end"), base + 3)]

            run, sends = own()
            needs = [("cast", g)]
            if order and GATE[order - 1]:
                needs += [(GATE[order - 1], GROUPS[order - 1], h) for h in (0, 1)]
            steps = [Step(run, sends=sends, needs=needs, gives=("own", g, half), rank=rank)]
            for side in ("+", "-"):
                run, sends = first(side)
                steps.append(Step(run, waits=(key("f", side),), sends=sends, rank=rank,
                                  gives=("near", g, half) if side == "-" else None))
            run, sends = far()
            steps.append(Step(run, waits=(key("f2"),), sends=sends, rank=rank, gives=("far", g, half)))
            lists.append(steps)
            steps = []
            for i in (0, 3, 1, 2):
                for side in ("+", "-"):
                    run, sends = second(i, side)
                    steps.append(Step(run, waits=(key("s", i, side),), sends=sends, rank=rank))
            steps[-1].gives = ("last", g, half)
            lists.append(steps)

        def end():
            got(wspan(g, 4), ("w", g), ("w", g, "end"))
        lists.append([Step(end, waits=(("w", g, "end"),), needs=(("last", g, 0), ("last", g, 1)), gives=("W", g), rank=rank)])

    for order, g in enumerate(GROUPS):
        weight_lists(order, g)

    def tables():
        loads["cos"].wait()
        loads["sin"].wait()
        n = lax.broadcasted_iota(jnp.int32, (LEN, LEN), 0)
        m = lax.broadcasted_iota(jnp.int32, (LEN, LEN), 1)
        distance = jnp.maximum(n - m, 0).astype(F32)
        DEC[...] = jnp.where(n >= m, jnp.exp(-decay[...].reshape(1, 1) * distance), 0.0) * (LEN ** -0.5)

    lists.append([Step(tables, waits=("hbm",), gives="tables", rank=3.0, cost=0.15)])

    def chunk_list(k):
        steps = []
        base = 0.0 + 0.01 * k
        seq, half = k * ROWS // LEN, k % (LEN // ROWS)

        for s in range(3):
            n = s * CHUNKS + k
            xg = XG.at[n]
            akey, rkey = ("a", n), ("r", n)

            def slot(t, n=n):
                return XG.at[n, t]

            def half_of(t, h, n=n):
                return XG.at[n, t, pl.ds(HALF * h, HALF), :]

            gains = s == 0 and k == 0

            def a0(s=s, akey=akey, slot=slot, gains=gains):
                if s == 0:
                    loads[("t", k)].wait()
                for way, r in (("x+", "L"), ("x-", "R"), ("d", "D")):
                    send(slot(tp), akey, akey + (r,), way)
                if gains:
                    for i, gain in enumerate((gain_one, gain_mix, gain_two)):
                        GB[tp, i : i + 1, :] = gain[...]
                    for way, r in (("x+", "L"), ("x-", "R"), ("d", "D")):
                        send(GB.at[tp], ("g",), ("g", r), way)

            def a1(akey=akey, slot=slot, half_of=half_of, gains=gains):
                t = tp_of(3, c)
                got(slot(t), akey, akey + ("L",))
                send(half_of(t, 0), akey, akey + ("F",), "x+")
                send(slot(t), akey, akey + ("D",), "d")
                if gains:
                    got(GB.at[t], ("g",), ("g", "L"))
                    send(GB.at[t], ("g",), ("g", "F"), "x+")
                    send(GB.at[t], ("g",), ("g", "D"), "d")

            def a2(akey=akey, slot=slot, half_of=half_of, gains=gains):
                t = tp_of(1, c)
                got(slot(t), akey, akey + ("R",))
                send(half_of(t, 1), akey, akey + ("F",), "x-")
                send(slot(t), akey, akey + ("D",), "d")
                if gains:
                    got(GB.at[t], ("g",), ("g", "R"))
                    send(GB.at[t], ("g",), ("g", "D"), "d")

            def a3(akey=akey, slot=slot, gains=gains):
                t = tp_of(2, c)
                got(slot(t), akey, akey + ("F",))
                send(slot(t), akey, akey + ("D",), "d")
                if gains:
                    got(GB.at[t], ("g",), ("g", "F"))
                    send(GB.at[t], ("g",), ("g", "D"), "d")

            def normed(n=n, s=s, akey=akey, gains=gains):
                got(XG.at[n, pl.ds(0, 4)], akey, akey + ("D",))
                if gains:
                    got(GB.at[pl.ds(0, 4)], ("g",), ("g", "D"))

                def rows_of(i, carry):
                    r = pl.ds(pl.multiple_of(i * 16, 16), 16)
                    hs = [XG[n, t, r, :].astype(F32) for t in range(8)]
                    squares = hs[0] * hs[0]
                    for h in hs[1:]:
                        squares += h * h
                    scale = lax.rsqrt(jnp.sum(squares, axis=1, keepdims=True) / D + EPS)
                    for t in range(8):
                        NX[k, r, 256 * t : 256 * t + 256] = (hs[t] * scale * GB[t, s : s + 1, :]).astype(BF16)
                    return carry

                lax.fori_loop(0, ROWS // 16, rows_of, 0, unroll=4)

            def gate_up():
                for j in range(3):
                    both = jnp.dot(NX[k], W_gu[:, 256 * j : 256 * j + 256], preferred_element_type=F32)
                    lane = slice(128 * j, 128 * j + 128)
                    gate = both[:, :128] * s_gate[lane].reshape(1, 128)
                    up = both[:, 128:] * s_up[lane].reshape(1, 128)
                    HID[k, :, lane] = (gate / (1.0 + jnp.exp(-gate)) * up).astype(BF16)

            def turned(v):
                at = slice(ROWS * half, ROWS * half + ROWS)
                even = lax.broadcasted_iota(jnp.int32, (ROWS, 256), 1) % 2 == 0
                swapped = jnp.where(even, -pltpu.roll(v, 255, 1), pltpu.roll(v, 1, 1))
                return (v * COS[at, :] + swapped * SIN[at, :]).astype(BF16)

            def query_key():
                at = slice(ROWS * half, ROWS * half + ROWS)
                for j, scale in enumerate((s_key, s_value, s_query, s_outgate)):
                    col = 256 * (1, 2, 0, 3)[j]
                    pre = jnp.dot(NX[k], W_qk[:, col : col + 256], preferred_element_type=F32)
                    row = (pre * scale[...]).astype(BF16)
                    if j == 0:
                        KB[seq, at, :] = turned(row.astype(F32))
                    elif j == 1:
                        VB[seq, at, :] = row
                    elif j == 2:
                        QB[k] = turned(row.astype(F32))
                    else:
                        OG[k] = row

            def retained():
                seen = ROWS * half + ROWS
                scores = lax.dot_general(
                    QB[k], KB[seq, 0:seen, :], (((1,), (1,)), ((), ())), preferred_element_type=F32
                )
                scores = scores * DEC[ROWS * half : seen, 0:seen]
                kept = jnp.dot(scores.astype(BF16), VB[seq, 0:seen, :], preferred_element_type=F32)
                kept = kept * lax.rsqrt(jnp.mean(kept * kept, axis=1, keepdims=True) + HEAD_EPS)
                gate = OG[k].astype(F32)
                MX[k] = (kept * ret_gain[...] * (gate / (1.0 + jnp.exp(-gate)))).astype(BF16)

            def product(i, core, s=s):
                cols = pl.ds(pl.multiple_of((around(x, i) * 2 + core) * 256, 256), 256)
                if s == 1:
                    return jnp.dot(MX[k], W_mx[:, cols], preferred_element_type=F32)
                return jnp.dot(HID[k], W_dn[:, cols], preferred_element_type=F32)

            def theirs(n=n, rkey=rkey, product=product):
                for i, r in ((2, "2"), (1, "13"), (3, "13"), (0, "0")):
                    PB[n, i] = product(i, 1 - c).astype(BF16)
                    send(PB.at[n, i], rkey, rkey + (r,), "d", RD.at[n, i])

            def mine(product=product):
                for i in (2, 1, 3, 0):
                    OB[k, i] = product(i, c)

            def r0(n=n, rkey=rkey):
                got(RD.at[n, 2], rkey, rkey + ("2",))
                SB[n, 0] = (OB[k, 2] + RD[n, 2].astype(F32)).astype(BF16)
                send(SB.at[n, 0, pl.ds(0, HALF)], rkey, rkey + ("L",), "x+", R1.at[n, 0])
                send(SB.at[n, 0, pl.ds(HALF, HALF)], rkey, rkey + ("R",), "x-", R1.at[n, 1])

            def r1(n=n, rkey=rkey):
                got(RD.at[n, pl.ds(0, 2)], rkey, rkey + ("13",))
                upper = OB[k, 1, HALF:ROWS] + RD[n, 1, HALF:ROWS].astype(F32)
                SB[n, 1, HALF:ROWS] = upper.astype(BF16)
                send(SB.at[n, 1, pl.ds(HALF, HALF)], rkey, rkey + ("E",), "x+", FIN.at[n, 0, pl.ds(HALF, HALF)])
                lower = OB[k, 3, 0:HALF] + RD[n, 3, 0:HALF].astype(F32)
                SB[n, 2, 0:HALF] = lower.astype(BF16)
                send(SB.at[n, 2, pl.ds(0, HALF)], rkey, rkey + ("E",), "x-", FIN.at[n, 1, pl.ds(0, HALF)])

            def r2(n=n, rkey=rkey):
                got(R1.at[n, 0], rkey, rkey + ("L",))
                SB[n, 1, 0:HALF] = (
                    OB[k, 1, 0:HALF] + RD[n, 1, 0:HALF].astype(F32) + R1[n, 0].astype(F32)
                ).astype(BF16)
                send(SB.at[n, 1, pl.ds(0, HALF)], rkey, rkey + ("E",), "x+", FIN.at[n, 0, pl.ds(0, HALF)])

            def r3(n=n, rkey=rkey):
                got(R1.at[n, 1], rkey, rkey + ("R",))
                SB[n, 2, HALF:ROWS] = (
                    OB[k, 3, HALF:ROWS] + RD[n, 3, HALF:ROWS].astype(F32) + R1[n, 1].astype(F32)
                ).astype(BF16)
                send(SB.at[n, 2, pl.ds(HALF, HALF)], rkey, rkey + ("E",), "x-", FIN.at[n, 1, pl.ds(HALF, HALF)])

            def r4(n=n, s=s, rkey=rkey):
                got(RD.at[n, 0], rkey, rkey + ("0",))
                got(FIN.at[n], rkey, rkey + ("E",))
                total = OB[k, 0] + RD[n, 0].astype(F32) + FIN[n, 0].astype(F32) + FIN[n, 1].astype(F32)
                if s == 1:
                    total = total * s_mix[...]
                else:
                    total = 0.5 * total * s_down[...]
                after = (XG[n, tp].astype(F32) + total).astype(BF16)
                if s < 2:
                    XG[n + CHUNKS, tp] = after
                else:
                    OUT[k] = after
                    pltpu.make_async_copy(OUT.at[k], out.at[pl.ds(k * ROWS, ROWS), :], hbm_sem.at[24 + k]).start()

            ua, ur = 2 * s * STAGE_GAP + k, (2 * s + 1) * STAGE_GAP + k
            base = 0.01 * ua
            L, R, F, Dk = (akey + (r,) for r in "LRFD")
            extra = (("g", "L"), ("g", "R"), ("g", "F"), ("g", "D"))
            sends = [("x+", BLOCK, L, ua), ("x-", BLOCK, R, ua), ("d", BLOCK, Dk, ua)]
            waits = ("hbm",) if s == 0 else ()
            gsize = 8192
            add = lambda *pairs: [(w, gsize, q, -1) for w, q in pairs] if gains else []
            more = lambda q: (q,) if gains else ()
            a0_step = Step(a0, waits=waits, sends=sends + add(("x+", extra[0]), ("x-", extra[1]), ("d", extra[3])),
                           rank=base + (0.0 if s else -1 + 0.1 * k))
            steps.append(a0_step)
            steps.append(Step(a1, waits=(L,) + more(extra[0]),
                              sends=[("x+", BLOCK // 2, F, ua), ("d", BLOCK, Dk, ua)] + add(("x+", extra[2]), ("d", extra[3])), rank=base))
            steps.append(Step(a2, waits=(R,) + more(extra[1]),
                              sends=[("x-", BLOCK // 2, F, ua), ("d", BLOCK, Dk, ua)] + add(("d", extra[3])), rank=base))
            steps.append(Step(a3, waits=(F,) + more(extra[2]), sends=[("d", BLOCK, Dk, ua)] + add(("d", extra[3])), rank=base))
            needs = ("gains",) if s == 0 and k else ()
            steps.append(Step(normed, waits=(Dk,) + more(extra[3]), needs=needs, gives="gains" if gains else None,
                              rank=2 + base, cost=COST["norm"]))
            if s == 1:
                steps.append(Step(query_key, needs=(("W", "qk"), "tables"), rank=2 + base, cost=COST["qk"], gives=("kv", k)))
                steps.append(Step(retained, needs=tuple(("kv", k - i) for i in range(half + 1)), rank=2 + base, cost=COST["ret"]))
                end, cost = ("W", "mx"), COST["mx"]
            else:
                steps.append(Step(gate_up, needs=(("W", "gu"),), rank=2 + base, cost=COST["gu"]))
                end, cost = ("W", "dn"), COST["dn"]
            r = lambda q: rkey + (q,)
            steps.append(Step(theirs, needs=(end,), rank=2 + base, cost=cost,
                              sends=[("d", BLOCK, r(q), ur) for q in ("2", "13", "13", "0")]))
            steps.append(Step(mine, rank=2 + base, cost=cost))
            steps.append(Step(r0, waits=(r("2"),), rank=base, sends=[("x+", BLOCK // 2, r("L"), ur), ("x-", BLOCK // 2, r("R"), ur)], cost=0.05))
            steps.append(Step(r1, waits=(r("13"),), rank=base, sends=[("x+", BLOCK // 2, r("E"), ur), ("x-", BLOCK // 2, r("E"), ur)], cost=0.05))
            steps.append(Step(r2, waits=(r("L"),), rank=base, sends=[("x+", BLOCK // 2, r("E"), ur)]))
            steps.append(Step(r3, waits=(r("R"),), rank=base, sends=[("x-", BLOCK // 2, r("E"), ur)]))
            steps.append(Step(r4, waits=(r("E"), r("0")), rank=base, cost=0.1))
        return steps

    for k in range(CHUNKS):
        lists.append(chunk_list(k))

    order = in_order(lists)
    pl.semaphore_wait(barrier, 7)
    for _, step, which in order:
        if which is None:
            held.clear()
            step.run()
            step.held = list(held)
            assert [w for w, _ in held] == [e[0] for e in step.sends]
        else:
            step.held[which][1]()

    for g in GROUPS:
        left(wspan(g, 15), ("w", g), ("w", g, "end"))
    left(GB.at[pl.ds(0, 7)], ("g",), ("g", "D"))
    for n in range(3 * CHUNKS):
        left(XG.at[n, pl.ds(0, 7)], ("a", n), ("a", n, "D"))
        left(XG.at[n, pl.ds(0, 7)], ("r", n), ("r", n, "0"))
    for k in range(CHUNKS):
        pltpu.make_async_copy(OUT.at[k], out.at[pl.ds(k * ROWS, ROWS), :], hbm_sem.at[24 + k]).wait()
    assert len(recv.at) <= NSEM_RECV and len(sent.at) <= NSEM_SEND


def per_device(
    tokens, gain_one, w_gate, w_up, w_down, scale_gate, scale_up, scale_down, gain_mix,
    w_query, w_key, w_value, w_outgate, scale_query, scale_key, scale_value, scale_outgate,
    ret_gain, decay_rate, w_mix, scale_mix, gain_two,
):
    freq = (1.0 / 10000.0 ** np.linspace(0.0, 1.0, 128)).astype(np.float32)
    angles = (np.arange(LEN, dtype=np.float32)[:, None] * np.repeat(freq, 2)[None, :]).astype(np.float64)
    cos_t = jnp.asarray(np.cos(angles), F32)
    sin_t = jnp.asarray(np.sin(angles), F32)
    row = lambda v: v.reshape(1, -1)
    small = [
        row(gain_one), row(gain_mix), row(gain_two), scale_gate, scale_up, row(scale_down), row(scale_query),
        row(scale_key), row(scale_value), row(scale_outgate), row(ret_gain), decay_rate, row(scale_mix),
    ]
    anywhere = pl.BlockSpec(memory_space=pl.ANY)
    vmem = pl.BlockSpec(memory_space=pltpu.VMEM)
    V = pltpu.VMEM
    hops = 3 * CHUNKS
    return pl.pallas_call(
        layer_kernel,
        out_shape=jax.ShapeDtypeStruct((CHUNKS * ROWS, 256), BF16),
        in_specs=[anywhere] * 11 + [vmem] * len(small),
        out_specs=anywhere,
        scratch_shapes=[
            V((2048, 768), BF16), V((384, 2048), BF16), V((2048, 1024), BF16), V((256, 2048), BF16),
            V((2, 128, 384), F32), V((384, 128), F32), V((4, 128, 256), F32), V((256, 128), F32),
            V((LEN, 256), F32), V((LEN, 256), F32), V((LEN, LEN), F32), V((8, 8, 256), F32),
            V((hops, 8, ROWS, 256), BF16), V((CHUNKS, ROWS, D), BF16), V((CHUNKS, ROWS, 384), BF16),
            V((CHUNKS, ROWS, 256), BF16), V((CHUNKS, ROWS, 256), BF16), V((CHUNKS * ROWS // LEN, LEN, 256), BF16),
            V((CHUNKS * ROWS // LEN, LEN, 256), BF16), V((CHUNKS, ROWS, 256), BF16), V((CHUNKS, 4, ROWS, 256), F32),
            V((hops, 4, ROWS, 256), BF16), V((hops, 4, ROWS, 256), BF16), V((hops, 3, ROWS, 256), BF16),
            V((hops, 2, HALF, 256), BF16), V((hops, 2, ROWS, 256), BF16), V((CHUNKS, ROWS, 256), BF16),
            pltpu.SemaphoreType.DMA((32,)), pltpu.SemaphoreType.DMA((NSEM_RECV,)), pltpu.SemaphoreType.DMA((NSEM_SEND,)),
        ],
        compiler_params=pltpu.CompilerParams(
            collective_id=0, has_side_effects=True, vmem_limit_bytes=60 * 1024 * 1024
        ),
        name="layer",
    )(tokens, w_gate, w_up, w_down, w_query, w_key, w_value, w_outgate, w_mix, cos_t, sin_t, *small)


def solution(mesh):
    return jax.shard_map(
        per_device,
        mesh=mesh,
        in_specs=(
            P("fs", "tp"), P("tp"), P("fs", "tp"), P("fs", "tp"), P("tp", "fs"), P("tp"), P("tp"), P("tp"), P("tp"),
            P("fs", "tp"), P("fs", "tp"), P("fs", "tp"), P("fs", "tp"), P("tp"), P("tp"), P("tp"), P("tp"), P("tp"),
            P("tp"), P("tp", "fs"), P("tp"), P("tp"),
        ),
        out_specs=P("fs", "tp"),
        check_vma=False,
    )
```

```python
import functools

import jax
import jax.numpy as jnp
import numpy as np
from jax import lax
from jax.experimental import pallas as pl
from jax.experimental.pallas import tpu as pltpu
from jax.sharding import PartitionSpec as P

MESH = pl.DeviceIdType.MESH
BF16 = jnp.bfloat16
F32 = jnp.float32

D = 2048
LEN = 256
ROWS = 128
HALF = ROWS // 2
CHUNKS = 6
EPS = 1e-06
HEAD_EPS = 0.1
GROUPS = ("gu", "dn", "qk", "mx")
PIECE_ROWS = {"gu": 128, "dn": 384, "qk": 128, "mx": 256}
PIECE_BYTES = {"gu": 196608, "dn": 98304, "qk": 262144, "mx": 65536}
BLOCK = ROWS * 512


class Step:
    def __init__(self, run, waits=(), sends=(), needs=(), gives=None, cost=0.02, rank=1.0):
        self.run, self.waits, self.sends = run, waits, sends
        self.needs, self.gives, self.cost, self.rank = needs, gives, cost, rank


START = 1.5
MARGIN = 0.0
LATENCY = 2.6
WAYS = ("x+", "x-", "d", "y+", "y-", "z+", "z-")
GROUP_BASE = (-1.25, 2.75, 8.25, 11.5)
WPRI = (-0.75, -1.5, -9.25, -7.5, 1.75)
XPRI = (-1.75, -1.0, -2.75, 2.0, 3.25, -4.0)
RANKS = (11.25, -0.8)
STAGE_GAP = 7.0
COST = {"norm": 0.37, "gu": 0.73, "qk": 0.83, "ret": 0.4, "dn": 0.32, "mx": 0.25}
GATE = (None, None, None)


def link_time(way, size):
    return size / (300e3 if way == "d" else 45.7e3)


def in_order(lists):
    clock, free, given, order = 0.0, {}, set(), []
    arrive = {"hbm": 0.5}
    for way in WAYS:
        free[way] = START
    pending = {way: [] for way in WAYS}
    heads = [0] * len(lists)
    count = 0

    def issue(way, entry):
        _, _, size, key, step, which = entry
        done = max(free[way], clock) + link_time(way, size)
        free[way] = done
        arrive[key] = max(arrive.get(key, 0.0), done + (0.9 if way == "d" else LATENCY))
        missing[key] -= 1
        order.append((clock, step, which))

    missing = {"hbm": 0}
    for steps in lists:
        for step in steps:
            for _, _, key, _ in step.sends:
                missing[key] = missing.get(key, 0) + 1

    while True:
        best = None
        for number, steps in enumerate(lists):
            if heads[number] == len(steps):
                continue
            step = steps[heads[number]]
            if any(k not in given for k in step.needs) or any(missing[k] for k in step.waits):
                continue
            ready = max([clock] + [arrive[k] for k in step.waits])
            score = (ready, step.rank, number)
            if best is None or score < best[0]:
                best = (score, number, step)
        horizon = 1e9 if best is None else best[0][0] + best[2].cost + MARGIN
        issued = False
        for way in WAYS:
            if pending[way] and (way == "d" or free[way] < horizon):
                pending[way].sort(key=lambda e: e[:2])
                issue(way, pending[way].pop(0))
                issued = True
        if issued:
            continue
        if best is None:
            break
        (ready, _, _), number, step = best
        heads[number] += 1
        clock = ready + step.cost
        if step.gives is not None:
            given.add(step.gives)
        order.append((clock, step, None))
        for which, (way, size, key, urgency) in enumerate(step.sends):
            pending[way].append((urgency, count, size, key, step, which))
            count += 1
    assert all(h == len(s) for h, s in zip(heads, lists))
    return order


class Sems:
    def __init__(self, ref):
        self.ref, self.at = ref, {}

    def __getitem__(self, key):
        if key not in self.at:
            self.at[key] = len(self.at)
        return self.ref.at[self.at[key]]


NSEM_RECV = 156
NSEM_SEND = 11
NLOADS = 16


def layer_kernel(
    tokens, w_gate, w_up, w_down, w_query, w_key, w_value, w_outgate, w_mix, cos_t, sin_t,
    gain_one, gain_mix, gain_two, s_gate, s_up, s_down, s_query, s_key, s_value, s_outgate,
    ret_gain, decay, s_mix,
    out,
    W_gu, W_dn, W_qk, W_mx,
    F_gu, F_dn, F_qk, F_mx,
    COS, SIN, DEC, GB, XG, NX, HID, QB, OG, KB, VB, MX, OB, PB, RD, SB, R1, FIN, OUT,
    hbm_sem, recv_sem, send_sem,
):
    fs, tp = lax.axis_index("fs"), lax.axis_index("tp")
    z, y = fs // 4, fs % 4
    x, c = tp // 2, tp % 2

    def around(v, k):
        return (v + k) % 4

    def fs_of(zz, yy):
        return zz * 4 + yy

    def tp_of(k, core):
        return around(x, k) * 2 + core

    where = {
        "x+": (fs, tp_of(1, c)), "x-": (fs, tp_of(3, c)), "d": (fs, x * 2 + (1 - c)),
        "y+": (fs_of(z, around(y, 1)), tp), "y-": (fs_of(z, around(y, 3)), tp),
        "z+": (fs_of(around(z, 1), y), tp), "z-": (fs_of(around(z, 3), y), tp),
    }
    W = {"gu": W_gu, "dn": W_dn, "qk": W_qk, "mx": W_mx}
    recv, sent = Sems(recv_sem), Sems(send_sem)

    def copy(src, dst, send_key, recv_key, way):
        return pltpu.make_async_remote_copy(
            src_ref=src, dst_ref=dst, send_sem=sent[send_key], recv_sem=recv[recv_key],
            device_id=where[way], device_id_type=MESH,
        )

    held = []

    def send(ref, send_key, recv_key, way, dst=None):
        held.append((way, lambda: copy(ref, ref if dst is None else dst, send_key, recv_key, way).start()))

    def got(ref, send_key, recv_key):
        copy(ref, ref, send_key, recv_key, "d").wait_recv()

    def left(ref, send_key, recv_key):
        copy(ref, ref, send_key, recv_key, "d").wait_send()

    loads = {}

    def load(key, src, dst):
        loads[key] = pltpu.make_async_copy(src, dst, hbm_sem.at[len(loads)])
        loads[key].start()

    load("g", w_gate, F_gu.at[0])
    load("u", w_up, F_gu.at[1])
    for k in range(CHUNKS):
        load(("t", k), tokens.at[pl.ds(k * ROWS, ROWS), :], XG.at[k, tp])
    load("d", w_down, F_dn)
    for n, w in enumerate((w_query, w_key, w_value, w_outgate)):
        load(("q", n), w, F_qk.at[n])
    load("m", w_mix, F_mx)
    load("cos", cos_t, COS)
    load("sin", sin_t, SIN)

    barrier = pltpu.get_barrier_semaphore()
    for way in WAYS:
        pl.semaphore_signal(barrier, inc=1, device_id=where[way], device_id_type=MESH)

    lists = []

    def wpart(g, f, half, quarter=None):
        n = PIECE_ROWS[g] // 2
        lo = n * half
        if quarter is not None:
            n //= 2
            lo += n * quarter
        if g in ("gu", "qk"):
            return W[g].at[pl.ds(pl.multiple_of(f * 128 + lo, 32), n), :]
        return W[g].at[pl.ds(lo, n), pl.ds(pl.multiple_of(f * 128, 128), 128)]

    def wspan(g, pieces):
        if g in ("gu", "qk"):
            return W[g].at[pl.ds(0, 128 * pieces), :]
        return W[g].at[:, pl.ds(0, 128 * pieces)]

    def cast_gu():
        loads["g"].wait()
        loads["u"].wait()
        rows = pl.ds(pl.multiple_of(fs * 128, 128), 128)
        for j in range(3):
            W_gu[rows, 256 * j : 256 * j + 128] = F_gu[0, :, 128 * j : 128 * j + 128].astype(BF16)
            W_gu[rows, 256 * j + 128 : 256 * j + 256] = F_gu[1, :, 128 * j : 128 * j + 128].astype(BF16)

    def cast_dn():
        loads["d"].wait()
        W_dn[:, pl.ds(pl.multiple_of(fs * 128, 128), 128)] = F_dn[...].astype(BF16)

    def cast_qk():
        rows = pl.ds(pl.multiple_of(fs * 128, 128), 128)
        for n in range(4):
            loads[("q", n)].wait()
            W_qk[rows, 256 * n : 256 * n + 256] = F_qk[n].astype(BF16)

    def cast_mx():
        loads["m"].wait()
        W_mx[:, pl.ds(pl.multiple_of(fs * 128, 128), 128)] = F_mx[...].astype(BF16)

    casts = {"gu": cast_gu, "dn": cast_dn, "qk": cast_qk, "mx": cast_mx}
    cast_steps = []
    for n, g in enumerate(GROUPS):
        cast_steps.append(Step(casts[g], waits=("hbm",), gives=("cast", g), cost=0.05, rank=-5 if n == 0 else 1.5))
    lists.append(cast_steps)

    def weight_lists(order, g):
        rank = RANKS[1] + 0.1 * order
        base = GROUP_BASE[order]
        for half in (0, 1):
            a, b = ("y", "z") if half == 0 else ("z", "y")

            def at(i, j, a=a):
                return fs_of(around(z, j), around(y, i)) if a == "y" else fs_of(around(z, i), around(y, j))

            full = PIECE_BYTES[g] // 2
            key = lambda *k, half=half: ("w", g, half) + k
            skey = ("w", g)

            def both(i, half=half, at=at, a=a, b=b, key=key, full=full):
                def run():
                    for way in (b + "+", b + "-"):
                        send(wpart(g, at(i, 0), half), skey, key("s", i, way[1]), way)
                return run, [(way, full, key("s", i, way[1]), base + WPRI[3 if i else 1]) for way in (b + "+", b + "-")]

            def own(half=half, at=at, a=a, b=b, key=key, full=full):
                more, extra = both(0)
                def run():
                    for way in (a + "+", a + "-"):
                        send(wpart(g, at(0, 0), half), skey, key("f", way[1]), way)
                    more()
                return run, [(way, full, key("f", way[1]), base + WPRI[0]) for way in (a + "+", a + "-")] + extra

            def first(side, half=half, at=at, a=a, b=b, key=key, full=full):
                i, back, q = (3, "+", 0) if side == "+" else (1, "-", 1)
                more, extra = both(i)
                def run():
                    got(wpart(g, at(i, 0), half), skey, key("f", side))
                    send(wpart(g, at(i, 0), half, q), skey, key("f2"), a + back)
                    more()
                return run, [(a + back, full // 2, key("f2"), base + WPRI[2])] + extra

            def far(half=half, at=at, a=a, b=b, key=key):
                more, extra = both(2)
                def run():
                    got(wpart(g, at(2, 0), half), skey, key("f2"))
                    more()
                return run, extra

            def second(i, side, half=half, at=at, a=a, b=b, key=key, full=full):
                j, back, q = (3, "+", 0) if side == "+" else (1, "-", 1)
                def run():
                    got(wpart(g, at(i, j), half), skey, key("s", i, side))
                    send(wpart(g, at(i, j), half, q), skey, ("w", g, "end"), b + back)
                return run, [(b + back, full // 2, ("w", g, "end"), base + WPRI[4])]

            run, sends = own()
            needs = [("cast", g)]
            if order and GATE[order - 1]:
                needs += [(GATE[order - 1], GROUPS[order - 1], h) for h in (0, 1)]
            steps = [Step(run, sends=sends, needs=needs, gives=("own", g, half), rank=rank)]
            for side in ("+", "-"):
                run, sends = first(side)
                steps.append(Step(run, waits=(key("f", side),), sends=sends, rank=rank,
                                  gives=("near", g, half) if side == "-" else None))
            run, sends = far()
            steps.append(Step(run, waits=(key("f2"),), sends=sends, rank=rank, gives=("far", g, half)))
            lists.append(steps)
            steps = []
            for i in (0, 3, 1, 2):
                for side in ("+", "-"):
                    run, sends = second(i, side)
                    steps.append(Step(run, waits=(key("s", i, side),), sends=sends, rank=rank))
            steps[-1].gives = ("last", g, half)
            lists.append(steps)

        def end():
            got(wspan(g, 4), ("w", g), ("w", g, "end"))
        lists.append([Step(end, waits=(("w", g, "end"),), needs=(("last", g, 0), ("last", g, 1)), gives=("W", g), rank=rank)])

    for order, g in enumerate(GROUPS):
        weight_lists(order, g)

    def tables():
        loads["cos"].wait()
        loads["sin"].wait()
        n = lax.broadcasted_iota(jnp.int32, (LEN, LEN), 0)
        m = lax.broadcasted_iota(jnp.int32, (LEN, LEN), 1)
        distance = jnp.maximum(n - m, 0).astype(F32)
        DEC[...] = jnp.where(n >= m, jnp.exp(-decay[...].reshape(1, 1) * distance), 0.0) * (LEN ** -0.5)

    lists.append([Step(tables, waits=("hbm",), gives="tables", rank=3.0, cost=0.15)])

    def chunk_list(k):
        steps = []
        base = 0.0 + 0.01 * k
        seq, half = k * ROWS // LEN, k % (LEN // ROWS)

        for s in range(3):
            n = s * CHUNKS + k
            xg = XG.at[n]
            akey, rkey = ("a", n), ("r", n)
            acode, rcode, asend, rsend = ("a", k), ("r", k), ("as", s), ("rs", s)

            def slot(t, n=n):
                return XG.at[n, t]

            def half_of(t, h, n=n):
                return XG.at[n, t, pl.ds(HALF * h, HALF), :]

            gains = s == 0 and k == 0

            def a0(s=s, akey=acode, asend=asend, slot=slot, gains=gains):
                if s == 0:
                    loads[("t", k)].wait()
                for way, r in (("x+", "L"), ("x-", "R"), ("d", "D")):
                    send(slot(tp), asend, akey + (r,), way)
                if gains:
                    for i, gain in enumerate((gain_one, gain_mix, gain_two)):
                        GB[tp, i : i + 1, :] = gain[...]
                    for way, r in (("x+", "L"), ("x-", "R"), ("d", "D")):
                        send(GB.at[tp], ("g",), ("g", r), way)

            def a1(akey=acode, asend=asend, slot=slot, half_of=half_of, gains=gains):
                t = tp_of(3, c)
                got(slot(t), asend, akey + ("L",))
                send(half_of(t, 0), asend, akey + ("F",), "x+")
                send(slot(t), asend, akey + ("D",), "d")
                if gains:
                    got(GB.at[t], ("g",), ("g", "L"))
                    send(GB.at[t], ("g",), ("g", "F"), "x+")
                    send(GB.at[t], ("g",), ("g", "D"), "d")

            def a2(akey=acode, asend=asend, slot=slot, half_of=half_of, gains=gains):
                t = tp_of(1, c)
                got(slot(t), asend, akey + ("R",))
                send(half_of(t, 1), asend, akey + ("F",), "x-")
                send(slot(t), asend, akey + ("D",), "d")
                if gains:
                    got(GB.at[t], ("g",), ("g", "R"))
                    send(GB.at[t], ("g",), ("g", "D"), "d")

            def a3(akey=acode, asend=asend, slot=slot, gains=gains):
                t = tp_of(2, c)
                got(slot(t), asend, akey + ("F",))
                send(slot(t), asend, akey + ("D",), "d")
                if gains:
                    got(GB.at[t], ("g",), ("g", "F"))
                    send(GB.at[t], ("g",), ("g", "D"), "d")

            def normed(n=n, s=s, akey=acode, asend=asend, gains=gains):
                got(XG.at[n, pl.ds(0, 4)], asend, akey + ("D",))
                if gains:
                    got(GB.at[pl.ds(0, 4)], ("g",), ("g", "D"))

                def rows_of(i, carry):
                    r = pl.ds(pl.multiple_of(i * 16, 16), 16)
                    hs = [XG[n, t, r, :].astype(F32) for t in range(8)]
                    squares = hs[0] * hs[0]
                    for h in hs[1:]:
                        squares += h * h
                    scale = lax.rsqrt(jnp.sum(squares, axis=1, keepdims=True) / D + EPS)
                    for t in range(8):
                        NX[k, r, 256 * t : 256 * t + 256] = (hs[t] * scale * GB[t, s : s + 1, :]).astype(BF16)
                    return carry

                lax.fori_loop(0, ROWS // 16, rows_of, 0, unroll=4)

            def gate_up():
                for j in range(3):
                    both = jnp.dot(NX[k], W_gu[:, 256 * j : 256 * j + 256], preferred_element_type=F32)
                    lane = slice(128 * j, 128 * j + 128)
                    gate = both[:, :128] * s_gate[lane].reshape(1, 128)
                    up = both[:, 128:] * s_up[lane].reshape(1, 128)
                    HID[k, :, lane] = (gate / (1.0 + jnp.exp(-gate)) * up).astype(BF16)

            def turned(v):
                at = slice(ROWS * half, ROWS * half + ROWS)
                even = lax.broadcasted_iota(jnp.int32, (ROWS, 256), 1) % 2 == 0
                swapped = jnp.where(even, -pltpu.roll(v, 255, 1), pltpu.roll(v, 1, 1))
                return (v * COS[at, :] + swapped * SIN[at, :]).astype(BF16)

            def query_key():
                at = slice(ROWS * half, ROWS * half + ROWS)
                for j, scale in enumerate((s_key, s_value, s_query, s_outgate)):
                    col = 256 * (1, 2, 0, 3)[j]
                    pre = jnp.dot(NX[k], W_qk[:, col : col + 256], preferred_element_type=F32)
                    row = (pre * scale[...]).astype(BF16)
                    if j == 0:
                        KB[seq, at, :] = turned(row.astype(F32))
                    elif j == 1:
                        VB[seq, at, :] = row
                    elif j == 2:
                        QB[k] = turned(row.astype(F32))
                    else:
                        OG[k] = row

            def retained():
                seen = ROWS * half + ROWS
                scores = lax.dot_general(
                    QB[k], KB[seq, 0:seen, :], (((1,), (1,)), ((), ())), preferred_element_type=F32
                )
                scores = scores * DEC[ROWS * half : seen, 0:seen]
                kept = jnp.dot(scores.astype(BF16), VB[seq, 0:seen, :], preferred_element_type=F32)
                kept = kept * lax.rsqrt(jnp.mean(kept * kept, axis=1, keepdims=True) + HEAD_EPS)
                gate = OG[k].astype(F32)
                MX[k] = (kept * ret_gain[...] * (gate / (1.0 + jnp.exp(-gate)))).astype(BF16)

            def product(i, core, s=s):
                cols = pl.ds(pl.multiple_of((around(x, i) * 2 + core) * 256, 256), 256)
                if s == 1:
                    return jnp.dot(MX[k], W_mx[:, cols], preferred_element_type=F32)
                return jnp.dot(HID[k], W_dn[:, cols], preferred_element_type=F32)

            def theirs(n=n, rkey=rcode, rsend=rsend, product=product):
                for i, r in ((2, "2"), (1, "13"), (3, "13"), (0, "0")):
                    PB[n, i] = product(i, 1 - c).astype(BF16)
                    send(PB.at[n, i], rsend, rkey + (r,), "d", RD.at[n, i])

            def mine(product=product):
                for i in (2, 1, 3, 0):
                    OB[k, i] = product(i, c)

            def r0(n=n, rkey=rcode, rsend=rsend):
                got(RD.at[n, 2], rsend, rkey + ("2",))
                SB[n, 0] = (OB[k, 2] + RD[n, 2].astype(F32)).astype(BF16)
                send(SB.at[n, 0, pl.ds(0, HALF)], rsend, rkey + ("L",), "x+", R1.at[n, 0])
                send(SB.at[n, 0, pl.ds(HALF, HALF)], rsend, rkey + ("R",), "x-", R1.at[n, 1])

            def r1(n=n, rkey=rcode, rsend=rsend):
                got(RD.at[n, pl.ds(0, 2)], rsend, rkey + ("13",))
                upper = OB[k, 1, HALF:ROWS] + RD[n, 1, HALF:ROWS].astype(F32)
                SB[n, 1, HALF:ROWS] = upper.astype(BF16)
                send(SB.at[n, 1, pl.ds(HALF, HALF)], rsend, rkey + ("E",), "x+", FIN.at[n, 0, pl.ds(HALF, HALF)])
                lower = OB[k, 3, 0:HALF] + RD[n, 3, 0:HALF].astype(F32)
                SB[n, 2, 0:HALF] = lower.astype(BF16)
                send(SB.at[n, 2, pl.ds(0, HALF)], rsend, rkey + ("E",), "x-", FIN.at[n, 1, pl.ds(0, HALF)])

            def r2(n=n, rkey=rcode, rsend=rsend):
                got(R1.at[n, 0], rsend, rkey + ("L",))
                SB[n, 1, 0:HALF] = (
                    OB[k, 1, 0:HALF] + RD[n, 1, 0:HALF].astype(F32) + R1[n, 0].astype(F32)
                ).astype(BF16)
                send(SB.at[n, 1, pl.ds(0, HALF)], rsend, rkey + ("E",), "x+", FIN.at[n, 0, pl.ds(0, HALF)])

            def r3(n=n, rkey=rcode, rsend=rsend):
                got(R1.at[n, 1], rsend, rkey + ("R",))
                SB[n, 2, HALF:ROWS] = (
                    OB[k, 3, HALF:ROWS] + RD[n, 3, HALF:ROWS].astype(F32) + R1[n, 1].astype(F32)
                ).astype(BF16)
                send(SB.at[n, 2, pl.ds(HALF, HALF)], rsend, rkey + ("E",), "x-", FIN.at[n, 1, pl.ds(HALF, HALF)])

            def r4(n=n, s=s, rkey=rcode, rsend=rsend):
                got(RD.at[n, 0], rsend, rkey + ("0",))
                got(FIN.at[n], rsend, rkey + ("E",))
                total = OB[k, 0] + RD[n, 0].astype(F32) + FIN[n, 0].astype(F32) + FIN[n, 1].astype(F32)
                if s == 1:
                    total = total * s_mix[...]
                else:
                    total = 0.5 * total * s_down[...]
                after = (XG[n, tp].astype(F32) + total).astype(BF16)
                if s < 2:
                    XG[n + CHUNKS, tp] = after
                else:
                    OUT[k * ROWS : k * ROWS + ROWS, :] = after
                    rows = pl.ds(k * ROWS, ROWS)
                    pltpu.make_async_copy(OUT.at[rows, :], out.at[rows, :], hbm_sem.at[NLOADS]).start()

            ua, ur = 2 * s * STAGE_GAP + k, (2 * s + 1) * STAGE_GAP + k
            base = 0.01 * ua
            L, R, F, Dk = (akey + (r,) for r in "LRFD")
            extra = (("g", "L"), ("g", "R"), ("g", "F"), ("g", "D"))
            sends = [("x+", BLOCK, L, ua + XPRI[0]), ("x-", BLOCK, R, ua + XPRI[0]), ("d", BLOCK, Dk, ua)]
            waits = ("hbm",) if s == 0 else ()
            gsize = 8192
            add = lambda *pairs: [(w, gsize, q, -1) for w, q in pairs] if gains else []
            more = lambda q: (q,) if gains else ()
            a0_step = Step(a0, waits=waits, sends=sends + add(("x+", extra[0]), ("x-", extra[1]), ("d", extra[3])),
                           rank=base + (0.0 if s else -1 + 0.1 * k))
            steps.append(a0_step)
            steps.append(Step(a1, waits=(L,) + more(extra[0]),
                              sends=[("x+", BLOCK // 2, F, ua + XPRI[1]), ("d", BLOCK, Dk, ua)] + add(("x+", extra[2]), ("d", extra[3])), rank=base))
            steps.append(Step(a2, waits=(R,) + more(extra[1]),
                              sends=[("x-", BLOCK // 2, F, ua + XPRI[1]), ("d", BLOCK, Dk, ua)] + add(("d", extra[3])), rank=base))
            steps.append(Step(a3, waits=(F,) + more(extra[2]), sends=[("d", BLOCK, Dk, ua)] + add(("d", extra[3])), rank=base))
            needs = ("gains",) if s == 0 and k else ()
            steps.append(Step(normed, waits=(Dk,) + more(extra[3]), needs=needs, gives="gains" if gains else None,
                              rank=RANKS[0] + base, cost=COST["norm"]))
            if s == 1:
                steps.append(Step(query_key, needs=(("W", "qk"), "tables"), rank=RANKS[0] + base, cost=COST["qk"], gives=("kv", k)))
                steps.append(Step(retained, needs=tuple(("kv", k - i) for i in range(half + 1)), rank=RANKS[0] + base, cost=COST["ret"]))
                end, cost = ("W", "mx"), COST["mx"]
            else:
                steps.append(Step(gate_up, needs=(("W", "gu"),), rank=RANKS[0] + base, cost=COST["gu"]))
                end, cost = ("W", "dn"), COST["dn"]
            r = lambda q: rkey + (q,)
            steps.append(Step(theirs, needs=(end,), rank=RANKS[0] + base, cost=cost,
                              sends=[("d", BLOCK, r(q), ur) for q in ("2", "13", "13", "0")]))
            steps.append(Step(mine, rank=RANKS[0] + base, cost=cost))
            steps.append(Step(r0, waits=(r("2"),), rank=base, sends=[("x+", BLOCK // 2, r("L"), ur + XPRI[2]), ("x-", BLOCK // 2, r("R"), ur + XPRI[2])], cost=0.05))
            steps.append(Step(r1, waits=(r("13"),), rank=base, sends=[(w, BLOCK // 2, r("E"), ur + XPRI[3]) for w in ("x+", "x-")], cost=0.05))
            steps.append(Step(r2, waits=(r("L"),), rank=base, sends=[("x+", BLOCK // 2, r("E"), ur + XPRI[4])]))
            steps.append(Step(r3, waits=(r("R"),), rank=base, sends=[("x-", BLOCK // 2, r("E"), ur + XPRI[4])]))
            steps.append(Step(r4, waits=(r("E"), r("0")), rank=base, cost=0.1))
        return steps

    for k in range(CHUNKS):
        lists.append(chunk_list(k))

    order = in_order(lists)
    pl.semaphore_wait(barrier, 7)
    for _, step, which in order:
        if which is None:
            held.clear()
            step.run()
            step.held = list(held)
            assert [w for w, _ in held] == [e[0] for e in step.sends]
        else:
            step.held[which][1]()

    for g in GROUPS:
        left(wspan(g, 15), ("w", g), ("w", g, "end"))
    left(GB.at[pl.ds(0, 7)], ("g",), ("g", "D"))
    for s in range(3):
        left(XG.at[pl.ds(0, CHUNKS), pl.ds(0, 7)], ("as", s), ("a", 0, "D"))
        left(XG.at[pl.ds(0, CHUNKS), pl.ds(0, 7)], ("rs", s), ("r", 0, "0"))
    pltpu.make_async_copy(OUT, out, hbm_sem.at[NLOADS]).wait()
    assert len(recv.at) == NSEM_RECV and len(sent.at) == NSEM_SEND and len(loads) == NLOADS


def per_device(
    tokens, gain_one, w_gate, w_up, w_down, scale_gate, scale_up, scale_down, gain_mix,
    w_query, w_key, w_value, w_outgate, scale_query, scale_key, scale_value, scale_outgate,
    ret_gain, decay_rate, w_mix, scale_mix, gain_two,
):
    freq = (1.0 / 10000.0 ** np.linspace(0.0, 1.0, 128)).astype(np.float32)
    angles = (np.arange(LEN, dtype=np.float32)[:, None] * np.repeat(freq, 2)[None, :]).astype(np.float64)
    cos_t = jnp.asarray(np.cos(angles), F32)
    sin_t = jnp.asarray(np.sin(angles), F32)
    row = lambda v: v.reshape(1, -1)
    small = [
        row(gain_one), row(gain_mix), row(gain_two), scale_gate, scale_up, row(scale_down), row(scale_query),
        row(scale_key), row(scale_value), row(scale_outgate), row(ret_gain), decay_rate, row(scale_mix),
    ]
    anywhere = pl.BlockSpec(memory_space=pl.ANY)
    vmem = pl.BlockSpec(memory_space=pltpu.VMEM)
    V = pltpu.VMEM
    hops = 3 * CHUNKS
    return pl.pallas_call(
        layer_kernel,
        out_shape=jax.ShapeDtypeStruct((CHUNKS * ROWS, 256), BF16),
        in_specs=[anywhere] * 11 + [vmem] * len(small),
        out_specs=anywhere,
        scratch_shapes=[
            V((2048, 768), BF16), V((384, 2048), BF16), V((2048, 1024), BF16), V((256, 2048), BF16),
            V((2, 128, 384), F32), V((384, 128), F32), V((4, 128, 256), F32), V((256, 128), F32),
            V((LEN, 256), F32), V((LEN, 256), F32), V((LEN, LEN), F32), V((8, 8, 256), F32),
            V((hops, 8, ROWS, 256), BF16), V((CHUNKS, ROWS, D), BF16), V((CHUNKS, ROWS, 384), BF16),
            V((CHUNKS, ROWS, 256), BF16), V((CHUNKS, ROWS, 256), BF16), V((CHUNKS * ROWS // LEN, LEN, 256), BF16),
            V((CHUNKS * ROWS // LEN, LEN, 256), BF16), V((CHUNKS, ROWS, 256), BF16), V((CHUNKS, 4, ROWS, 256), F32),
            V((hops, 4, ROWS, 256), BF16), V((hops, 4, ROWS, 256), BF16), V((hops, 3, ROWS, 256), BF16),
            V((hops, 2, HALF, 256), BF16), V((hops, 2, ROWS, 256), BF16), V((CHUNKS * ROWS, 256), BF16),
            pltpu.SemaphoreType.DMA((NLOADS + 1,)), pltpu.SemaphoreType.DMA((NSEM_RECV,)), pltpu.SemaphoreType.DMA((NSEM_SEND,)),
        ],
        compiler_params=pltpu.CompilerParams(
            collective_id=0, has_side_effects=True, vmem_limit_bytes=60 * 1024 * 1024
        ),
        name="layer",
    )(tokens, w_gate, w_up, w_down, w_query, w_key, w_value, w_outgate, w_mix, cos_t, sin_t, *small)


def solution(mesh):
    return jax.shard_map(
        per_device,
        mesh=mesh,
        in_specs=(
            P("fs", "tp"), P("tp"), P("fs", "tp"), P("fs", "tp"), P("tp", "fs"), P("tp"), P("tp"), P("tp"), P("tp"),
            P("fs", "tp"), P("fs", "tp"), P("fs", "tp"), P("fs", "tp"), P("tp"), P("tp"), P("tp"), P("tp"), P("tp"),
            P("tp"), P("tp", "fs"), P("tp"), P("tp"),
        ),
        out_specs=P("fs", "tp"),
        check_vma=False,
    )
```

```python
import functools

import jax
import jax.numpy as jnp
import numpy as np
from jax import lax
from jax.experimental import pallas as pl
from jax.experimental.pallas import tpu as pltpu
from jax.sharding import PartitionSpec as P

MESH = pl.DeviceIdType.MESH
BF16 = jnp.bfloat16
F32 = jnp.float32

D = 2048
LEN = 256
ROWS = 128
HALF = ROWS // 2
CHUNKS = 6
EPS = 1e-06
HEAD_EPS = 0.1
GROUPS = ("gu", "dn", "qk", "mx")
PIECE_ROWS = {"gu": 128, "dn": 384, "qk": 128, "mx": 256}
PIECE_BYTES = {"gu": 196608, "dn": 98304, "qk": 262144, "mx": 65536}
BLOCK = ROWS * 512


class Step:
    def __init__(self, run, waits=(), sends=(), needs=(), gives=None, cost=0.02, rank=1.0):
        self.run, self.waits, self.sends = run, waits, sends
        self.needs, self.gives, self.cost, self.rank = needs, gives, cost, rank


START = 0.7
MARGIN = 0.1
LATENCY = 2.6
PARTNER = 1.7
WAYS = ("x+", "x-", "d", "y+", "y-", "z+", "z-")
GROUP_BASE = (5.25, 5.75, 7.25, 9.25)
WPRI = (-0.5, -1.0, -13.75, -2.5, 0.25)
XPRI = (0.25, -3.75, 1.25, -1.0, 2.75, -11.5)
RANKS = (26.5, 0.45)
STAGE_GAP = 10.0
COST = {"norm": 0.37, "gu": 0.73, "qk": 0.83, "ret": 0.4, "dn": 0.32, "mx": 0.25}
GATE = (None, None, None)


def link_time(way, size):
    return size / (300e3 if way == "d" else 45.7e3)


def in_order(lists):
    clock, free, given, order = 0.0, {}, set(), []
    arrive = {"hbm": 0.3}
    for way in WAYS:
        free[way] = START
    pending = {way: [] for way in WAYS}
    heads = [0] * len(lists)
    count = 0

    def issue(way, entry):
        _, _, size, key, step, which = entry
        done = max(free[way], clock) + link_time(way, size)
        free[way] = done
        arrive[key] = max(arrive.get(key, 0.0), done + (PARTNER if way == "d" else LATENCY))
        missing[key] -= 1
        order.append((clock, step, which))

    missing = {"hbm": 0}
    for steps in lists:
        for step in steps:
            for _, _, key, _ in step.sends:
                missing[key] = missing.get(key, 0) + 1

    while True:
        best = None
        for number, steps in enumerate(lists):
            if heads[number] == len(steps):
                continue
            step = steps[heads[number]]
            if any(k not in given for k in step.needs) or any(missing[k] for k in step.waits):
                continue
            ready = max([clock] + [arrive[k] for k in step.waits])
            score = (ready, step.rank, number)
            if best is None or score < best[0]:
                best = (score, number, step)
        horizon = 1e9 if best is None else best[0][0] + best[2].cost + MARGIN
        issued = False
        for way in WAYS:
            if pending[way] and (way == "d" or free[way] < horizon):
                pending[way].sort(key=lambda e: e[:2])
                issue(way, pending[way].pop(0))
                issued = True
        if issued:
            continue
        if best is None:
            break
        (ready, _, _), number, step = best
        heads[number] += 1
        clock = ready + step.cost
        if step.gives is not None:
            given.add(step.gives)
        order.append((clock, step, None))
        for which, (way, size, key, urgency) in enumerate(step.sends):
            pending[way].append((urgency, count, size, key, step, which))
            count += 1
    assert all(h == len(s) for h, s in zip(heads, lists))
    return order


class Sems:
    def __init__(self, ref):
        self.ref, self.at = ref, {}

    def __getitem__(self, key):
        if key not in self.at:
            self.at[key] = len(self.at)
        return self.ref.at[self.at[key]]


NSEM_RECV = 103
NSEM_SEND = 11
NLOADS = 11


def layer_kernel(
    tokens, w_gate, w_up, w_down, w_query, w_key, w_value, w_outgate, w_mix, cos_t, sin_t,
    gain_one, gain_mix, gain_two, s_gate, s_up, s_down, s_query, s_key, s_value, s_outgate,
    ret_gain, decay, s_mix,
    out,
    W_gu, W_dn, W_qk, W_mx,
    F_gu, F_dn, F_qk, F_mx,
    TURN, DEC, GB, XG, NX, HID, QB, OG, KB, VB, MX, OB, PB, RD, SB, R1, FIN, OUT,
    hbm_sem, recv_sem, send_sem,
):
    fs, tp = lax.axis_index("fs"), lax.axis_index("tp")
    z, y = fs // 4, fs % 4
    x, c = tp // 2, tp % 2

    def around(v, k):
        return (v + k) % 4

    def fs_of(zz, yy):
        return zz * 4 + yy

    def tp_of(k, core):
        return around(x, k) * 2 + core

    where = {
        "x+": (fs, tp_of(1, c)), "x-": (fs, tp_of(3, c)), "d": (fs, x * 2 + (1 - c)),
        "y+": (fs_of(z, around(y, 1)), tp), "y-": (fs_of(z, around(y, 3)), tp),
        "z+": (fs_of(around(z, 1), y), tp), "z-": (fs_of(around(z, 3), y), tp),
    }
    W = {"gu": W_gu, "dn": W_dn, "qk": W_qk, "mx": W_mx}
    recv, sent = Sems(recv_sem), Sems(send_sem)

    def copy(src, dst, send_key, recv_key, way):
        return pltpu.make_async_remote_copy(
            src_ref=src, dst_ref=dst, send_sem=sent[send_key], recv_sem=recv[recv_key],
            device_id=where[way], device_id_type=MESH,
        )

    held = []

    def send(ref, send_key, recv_key, way, dst=None):
        held.append((way, lambda: copy(ref, ref if dst is None else dst, send_key, recv_key, way).start()))

    def got(ref, send_key, recv_key):
        copy(ref, ref, send_key, recv_key, "d").wait_recv()

    def left(ref, send_key, recv_key):
        copy(ref, ref, send_key, recv_key, "d").wait_send()

    loads = {}

    def load(key, src, dst):
        loads[key] = pltpu.make_async_copy(src, dst, hbm_sem.at[len(loads)])
        loads[key].start()

    def load_all(key, sources, dst):
        at = len(loads)
        loads[key] = pltpu.make_async_copy(dst, dst, hbm_sem.at[at])
        for n, src in enumerate(sources):
            pltpu.make_async_copy(src, dst.at[n], hbm_sem.at[at]).start()

    load_all("gu", (w_gate, w_up), F_gu)
    for k in range(CHUNKS):
        load(("t", k), tokens.at[pl.ds(k * ROWS, ROWS), :], XG.at[k, tp])
    load("d", w_down, F_dn)
    load_all("q", (w_query, w_key, w_value, w_outgate), F_qk)
    load("m", w_mix, F_mx)
    load_all("turn", (cos_t, sin_t), TURN)

    barrier = pltpu.get_barrier_semaphore()
    for way in WAYS:
        pl.semaphore_signal(barrier, inc=1, device_id=where[way], device_id_type=MESH)

    lists = []

    def wpart(g, f, half, quarter=None):
        n = PIECE_ROWS[g] // 2
        lo = n * half
        if quarter is not None:
            n //= 2
            lo += n * quarter
        if g in ("gu", "qk"):
            return W[g].at[pl.ds(pl.multiple_of(f * 128 + lo, 32), n), :]
        return W[g].at[pl.ds(lo, n), pl.ds(pl.multiple_of(f * 128, 128), 128)]

    def wspan(g, pieces):
        if g in ("gu", "qk"):
            return W[g].at[pl.ds(0, 128 * pieces), :]
        return W[g].at[:, pl.ds(0, 128 * pieces)]

    def cast_gu():
        loads["gu"].wait()
        rows = pl.ds(pl.multiple_of(fs * 128, 128), 128)
        for j in range(3):
            W_gu[rows, 256 * j : 256 * j + 128] = F_gu[0, :, 128 * j : 128 * j + 128].astype(BF16)
            W_gu[rows, 256 * j + 128 : 256 * j + 256] = F_gu[1, :, 128 * j : 128 * j + 128].astype(BF16)

    def cast_dn():
        loads["d"].wait()
        W_dn[:, pl.ds(pl.multiple_of(fs * 128, 128), 128)] = F_dn[...].astype(BF16)

    def cast_qk():
        rows = pl.ds(pl.multiple_of(fs * 128, 128), 128)
        loads["q"].wait()
        for n in range(4):
            W_qk[rows, 256 * n : 256 * n + 256] = F_qk[n].astype(BF16)

    def cast_mx():
        loads["m"].wait()
        W_mx[:, pl.ds(pl.multiple_of(fs * 128, 128), 128)] = F_mx[...].astype(BF16)

    casts = {"gu": cast_gu, "dn": cast_dn, "qk": cast_qk, "mx": cast_mx}
    cast_steps = []
    for n, g in enumerate(GROUPS):
        cast_steps.append(Step(casts[g], waits=("hbm",), gives=("cast", g), cost=0.05, rank=-5 if n == 0 else 1.5))
    lists.append(cast_steps)

    def weight_lists(order, g):
        rank = RANKS[1] + 0.1 * order
        base = GROUP_BASE[order]
        for half in (0, 1):
            a, b = ("y", "z") if half == 0 else ("z", "y")

            def at(i, j, a=a):
                return fs_of(around(z, j), around(y, i)) if a == "y" else fs_of(around(z, i), around(y, j))

            full = PIECE_BYTES[g] // 2
            key = lambda *k, half=half: ("w", g, half) + k
            skey = ("w", g)

            def both(i, half=half, at=at, a=a, b=b, key=key, full=full):
                def run():
                    for way in (b + "+", b + "-"):
                        send(wpart(g, at(i, 0), half), skey, key("s", i), way)
                return run, [(way, full, key("s", i), base + WPRI[3 if i else 1]) for way in (b + "+", b + "-")]

            def own(half=half, at=at, a=a, b=b, key=key, full=full):
                more, extra = both(0)
                def run():
                    for way in (a + "+", a + "-"):
                        send(wpart(g, at(0, 0), half), skey, key("f"), way)
                    more()
                return run, [(way, full, key("f"), base + WPRI[0]) for way in (a + "+", a + "-")] + extra

            def first(half=half, at=at, a=a, b=b, key=key, full=full):
                (one, extra_one), (two, extra_two) = both(3), both(1)
                def run():
                    got(wspan(g, 1), skey, key("f"))
                    for i, back, q in ((3, "+", 0), (1, "-", 1)):
                        send(wpart(g, at(i, 0), half, q), skey, key("f2"), a + back)
                    one()
                    two()
                return run, [(a + back, full // 2, key("f2"), base + WPRI[2]) for back in "+-"] + extra_one + extra_two

            def far(half=half, at=at, a=a, b=b, key=key):
                more, extra = both(2)
                def run():
                    got(wpart(g, at(2, 0), half), skey, key("f2"))
                    more()
                return run, extra

            def second(i, half=half, at=at, a=a, b=b, key=key, full=full):
                def run():
                    got(wspan(g, 1), skey, key("s", i))
                    for j, back, q in ((3, "+", 0), (1, "-", 1)):
                        send(wpart(g, at(i, j), half, q), skey, ("w", g, "end"), b + back)
                return run, [(b + back, full // 2, ("w", g, "end"), base + WPRI[4]) for back in "+-"]

            run, sends = own()
            needs = [("cast", g)]
            if order and GATE[order - 1]:
                needs += [(GATE[order - 1], GROUPS[order - 1], h) for h in (0, 1)]
            steps = [Step(run, sends=sends, needs=needs, gives=("own", g, half), rank=rank)]
            run, sends = first()
            steps.append(Step(run, waits=(key("f"),), sends=sends, rank=rank, gives=("near", g, half)))
            run, sends = far()
            steps.append(Step(run, waits=(key("f2"),), sends=sends, rank=rank, gives=("far", g, half)))
            lists.append(steps)
            steps = []
            for i in (0, 3, 1, 2):
                run, sends = second(i)
                steps.append(Step(run, waits=(key("s", i),), sends=sends, rank=rank))
            steps[-1].gives = ("last", g, half)
            lists.append(steps)

        def end():
            got(wspan(g, 4), ("w", g), ("w", g, "end"))
        lists.append([Step(end, waits=(("w", g, "end"),), needs=(("last", g, 0), ("last", g, 1)), gives=("W", g), rank=rank)])

    for order, g in enumerate(GROUPS):
        weight_lists(order, g)

    def tables():
        loads["turn"].wait()
        n = lax.broadcasted_iota(jnp.int32, (LEN, LEN), 0)
        m = lax.broadcasted_iota(jnp.int32, (LEN, LEN), 1)
        distance = jnp.maximum(n - m, 0).astype(F32)
        DEC[...] = jnp.where(n >= m, jnp.exp(-decay[...].reshape(1, 1) * distance), 0.0) * (LEN ** -0.5)

    lists.append([Step(tables, waits=("hbm",), gives="tables", rank=3.0, cost=0.15)])

    def chunk_list(k):
        steps = []
        base = 0.0 + 0.01 * k
        seq, half = k * ROWS // LEN, k % (LEN // ROWS)

        for s in range(3):
            n = s * CHUNKS + k
            xg = XG.at[n]
            akey, rkey = ("a", n), ("r", n)
            acode, rcode, asend, rsend = ("a", k), ("r", k), ("as", s), ("rs", s)

            def slot(t, n=n):
                return XG.at[n, t]

            def half_of(t, h, n=n):
                return XG.at[n, t, pl.ds(HALF * h, HALF), :]

            gains = s == 0 and k == 0

            def a0(s=s, akey=acode, asend=asend, slot=slot, gains=gains):
                if s == 0:
                    loads[("t", k)].wait()
                for way, r in (("x+", "L"), ("x-", "L"), ("d", "D")):
                    send(slot(tp), asend, akey + (r,), way)
                if gains:
                    for i, gain in enumerate((gain_one, gain_mix, gain_two)):
                        GB[tp, i : i + 1, :] = gain[...]
                    for way, r in (("x+", "L"), ("x-", "L"), ("d", "D")):
                        send(GB.at[tp], ("g",), ("g", r), way)

            def a1(akey=acode, asend=asend, slot=slot, half_of=half_of, n=n, gains=gains):
                got(XG.at[n, pl.ds(0, 2)], asend, akey + ("L",))
                before, after = tp_of(3, c), tp_of(1, c)
                send(half_of(before, 0), asend, akey + ("F",), "x+")
                send(half_of(after, 1), asend, akey + ("F",), "x-")
                send(slot(before), asend, akey + ("D",), "d")
                send(slot(after), asend, akey + ("D",), "d")
                if gains:
                    got(GB.at[pl.ds(0, 2)], ("g",), ("g", "L"))
                    send(GB.at[before], ("g",), ("g", "F"), "x+")
                    send(GB.at[before], ("g",), ("g", "D"), "d")
                    send(GB.at[after], ("g",), ("g", "D"), "d")

            def a3(akey=acode, asend=asend, slot=slot, gains=gains):
                t = tp_of(2, c)
                got(slot(t), asend, akey + ("F",))
                send(slot(t), asend, akey + ("D",), "d")
                if gains:
                    got(GB.at[t], ("g",), ("g", "F"))
                    send(GB.at[t], ("g",), ("g", "D"), "d")

            def normed(n=n, s=s, akey=acode, asend=asend, gains=gains):
                got(XG.at[n, pl.ds(0, 4)], asend, akey + ("D",))
                if gains:
                    got(GB.at[pl.ds(0, 4)], ("g",), ("g", "D"))

                def rows_of(i, carry):
                    r = pl.ds(pl.multiple_of(i * 16, 16), 16)
                    hs = [XG[n, t, r, :].astype(F32) for t in range(8)]
                    squares = hs[0] * hs[0]
                    for h in hs[1:]:
                        squares += h * h
                    scale = lax.rsqrt(jnp.sum(squares, axis=1, keepdims=True) / D + EPS)
                    for t in range(8):
                        NX[k, r, 256 * t : 256 * t + 256] = (hs[t] * scale * GB[t, s : s + 1, :]).astype(BF16)
                    return carry

                lax.fori_loop(0, ROWS // 16, rows_of, 0, unroll=4)

            def gate_up():
                for j in range(3):
                    both = jnp.dot(NX[k], W_gu[:, 256 * j : 256 * j + 256], preferred_element_type=F32)
                    lane = slice(128 * j, 128 * j + 128)
                    gate = both[:, :128] * s_gate[lane].reshape(1, 128)
                    up = both[:, 128:] * s_up[lane].reshape(1, 128)
                    HID[k, :, lane] = (gate / (1.0 + jnp.exp(-gate)) * up).astype(BF16)

            def turned(v):
                at = slice(ROWS * half, ROWS * half + ROWS)
                even = lax.broadcasted_iota(jnp.int32, (ROWS, 256), 1) % 2 == 0
                swapped = jnp.where(even, -pltpu.roll(v, 255, 1), pltpu.roll(v, 1, 1))
                return (v * TURN[0, at, :] + swapped * TURN[1, at, :]).astype(BF16)

            def query_key():
                at = slice(ROWS * half, ROWS * half + ROWS)
                for j, scale in enumerate((s_key, s_value, s_query, s_outgate)):
                    col = 256 * (1, 2, 0, 3)[j]
                    pre = jnp.dot(NX[k], W_qk[:, col : col + 256], preferred_element_type=F32)
                    row = (pre * scale[...]).astype(BF16)
                    if j == 0:
                        KB[seq, at, :] = turned(row.astype(F32))
                    elif j == 1:
                        VB[seq, at, :] = row
                    elif j == 2:
                        QB[k] = turned(row.astype(F32))
                    else:
                        OG[k] = row

            def retained():
                seen = ROWS * half + ROWS
                scores = lax.dot_general(
                    QB[k], KB[seq, 0:seen, :], (((1,), (1,)), ((), ())), preferred_element_type=F32
                )
                scores = scores * DEC[ROWS * half : seen, 0:seen]
                kept = jnp.dot(scores.astype(BF16), VB[seq, 0:seen, :], preferred_element_type=F32)
                kept = kept * lax.rsqrt(jnp.mean(kept * kept, axis=1, keepdims=True) + HEAD_EPS)
                gate = OG[k].astype(F32)
                MX[k] = (kept * ret_gain[...] * (gate / (1.0 + jnp.exp(-gate)))).astype(BF16)

            def product(i, core, s=s):
                cols = pl.ds(pl.multiple_of((around(x, i) * 2 + core) * 256, 256), 256)
                if s == 1:
                    return jnp.dot(MX[k], W_mx[:, cols], preferred_element_type=F32)
                return jnp.dot(HID[k], W_dn[:, cols], preferred_element_type=F32)

            def theirs(n=n, rkey=rcode, rsend=rsend, product=product):
                for i, r in ((2, "2"), (1, "13"), (3, "13"), (0, "0")):
                    PB[n, i] = product(i, 1 - c).astype(BF16)
                    send(PB.at[n, i], rsend, rkey + (r,), "d", RD.at[n, i])

            def mine(product=product):
                for i in (2, 1, 3, 0):
                    OB[k, i] = product(i, c)

            def r0(n=n, rkey=rcode, rsend=rsend):
                got(RD.at[n, 2], rsend, rkey + ("2",))
                SB[n, 0] = (OB[k, 2] + RD[n, 2].astype(F32)).astype(BF16)
                send(SB.at[n, 0, pl.ds(0, HALF)], rsend, rkey + ("L",), "x+", R1.at[n, 0])
                send(SB.at[n, 0, pl.ds(HALF, HALF)], rsend, rkey + ("L",), "x-", R1.at[n, 1])

            def r1(n=n, rkey=rcode, rsend=rsend):
                got(RD.at[n, pl.ds(0, 2)], rsend, rkey + ("13",))
                upper = OB[k, 1, HALF:ROWS] + RD[n, 1, HALF:ROWS].astype(F32)
                SB[n, 1, HALF:ROWS] = upper.astype(BF16)
                send(SB.at[n, 1, pl.ds(HALF, HALF)], rsend, rkey + ("E",), "x+", FIN.at[n, 0, pl.ds(HALF, HALF)])
                lower = OB[k, 3, 0:HALF] + RD[n, 3, 0:HALF].astype(F32)
                SB[n, 2, 0:HALF] = lower.astype(BF16)
                send(SB.at[n, 2, pl.ds(0, HALF)], rsend, rkey + ("E",), "x-", FIN.at[n, 1, pl.ds(0, HALF)])

            def r2(n=n, rkey=rcode, rsend=rsend):
                got(R1.at[n], rsend, rkey + ("L",))
                SB[n, 1, 0:HALF] = (
                    OB[k, 1, 0:HALF] + RD[n, 1, 0:HALF].astype(F32) + R1[n, 0].astype(F32)
                ).astype(BF16)
                send(SB.at[n, 1, pl.ds(0, HALF)], rsend, rkey + ("E",), "x+", FIN.at[n, 0, pl.ds(0, HALF)])
                SB[n, 2, HALF:ROWS] = (
                    OB[k, 3, HALF:ROWS] + RD[n, 3, HALF:ROWS].astype(F32) + R1[n, 1].astype(F32)
                ).astype(BF16)
                send(SB.at[n, 2, pl.ds(HALF, HALF)], rsend, rkey + ("E",), "x-", FIN.at[n, 1, pl.ds(HALF, HALF)])

            def r4(n=n, s=s, rkey=rcode, rsend=rsend):
                got(RD.at[n, 0], rsend, rkey + ("0",))
                got(FIN.at[n], rsend, rkey + ("E",))
                total = OB[k, 0] + RD[n, 0].astype(F32) + FIN[n, 0].astype(F32) + FIN[n, 1].astype(F32)
                if s == 1:
                    total = total * s_mix[...]
                else:
                    total = 0.5 * total * s_down[...]
                after = (XG[n, tp].astype(F32) + total).astype(BF16)
                if s < 2:
                    XG[n + CHUNKS, tp] = after
                else:
                    OUT[k * ROWS : k * ROWS + ROWS, :] = after
                    rows = pl.ds(k * ROWS, ROWS)
                    pltpu.make_async_copy(OUT.at[rows, :], out.at[rows, :], hbm_sem.at[NLOADS]).start()

            ua, ur = 2 * s * STAGE_GAP + k, (2 * s + 1) * STAGE_GAP + k
            base = 0.01 * ua
            L, F, Dk = (akey + (r,) for r in "LFD")
            extra = {r: ("g", r) for r in "LFD"}
            sends = [("x+", BLOCK, L, ua + XPRI[0]), ("x-", BLOCK, L, ua + XPRI[0]), ("d", BLOCK, Dk, ua)]
            waits = ("hbm",) if s == 0 else ()
            add = lambda *pairs: [(w, 8192, extra[q], -9) for w, q in pairs] if gains else []
            more = lambda q: (extra[q],) if gains else ()
            steps.append(Step(a0, waits=waits, sends=sends + add(("x+", "L"), ("x-", "L"), ("d", "D")),
                              rank=base + (0.0 if s else -1 + 0.1 * k)))
            sends = [("x+", BLOCK // 2, F, ua + XPRI[1]), ("x-", BLOCK // 2, F, ua + XPRI[1])] + 2 * [("d", BLOCK, Dk, ua)]
            steps.append(Step(a1, waits=(L,) + more("L"), sends=sends + add(("x+", "F"), ("d", "D"), ("d", "D")), rank=base))
            steps.append(Step(a3, waits=(F,) + more("F"), sends=[("d", BLOCK, Dk, ua)] + add(("d", "D")), rank=base))
            needs = ("gains",) if s == 0 and k else ()
            steps.append(Step(normed, waits=(Dk,) + more("D"), needs=needs, gives="gains" if gains else None,
                              rank=RANKS[0] + base, cost=COST["norm"]))
            if s == 1:
                steps.append(Step(query_key, needs=(("W", "qk"), "tables"), rank=RANKS[0] + base, cost=COST["qk"], gives=("kv", k)))
                steps.append(Step(retained, needs=tuple(("kv", k - i) for i in range(half + 1)), rank=RANKS[0] + base, cost=COST["ret"]))
                end, cost = ("W", "mx"), COST["mx"]
            else:
                steps.append(Step(gate_up, needs=(("W", "gu"),), rank=RANKS[0] + base, cost=COST["gu"]))
                end, cost = ("W", "dn"), COST["dn"]
            r = lambda q: rkey + (q,)
            steps.append(Step(theirs, needs=(end,), rank=RANKS[0] + base, cost=cost,
                              sends=[("d", BLOCK, r(q), ur) for q in ("2", "13", "13", "0")]))
            steps.append(Step(mine, rank=RANKS[0] + base, cost=cost))
            two = lambda q, i: [(w, BLOCK // 2, r(q), ur + XPRI[i]) for w in ("x+", "x-")]
            steps.append(Step(r0, waits=(r("2"),), rank=base, sends=two("L", 2), cost=0.03))
            steps.append(Step(r1, waits=(r("13"),), rank=base, sends=two("E", 3), cost=0.03))
            steps.append(Step(r2, waits=(r("L"),), rank=base, sends=two("E", 4), cost=0.05))
            steps.append(Step(r4, waits=(r("E"), r("0")), rank=base, cost=0.1))
        return steps

    for k in range(CHUNKS):
        lists.append(chunk_list(k))

    order = in_order(lists)
    pl.semaphore_wait(barrier, 7)
    for _, step, which in order:
        if which is None:
            held.clear()
            step.run()
            step.held = list(held)
            assert [w for w, _ in held] == [e[0] for e in step.sends]
        else:
            step.held[which][1]()

    for g in GROUPS:
        left(wspan(g, 15), ("w", g), ("w", g, "end"))
    left(GB.at[pl.ds(0, 7)], ("g",), ("g", "D"))
    for s in range(3):
        left(XG.at[pl.ds(0, CHUNKS), pl.ds(0, 7)], ("as", s), ("a", 0, "D"))
        left(XG.at[pl.ds(0, CHUNKS), pl.ds(0, 7)], ("rs", s), ("r", 0, "0"))
    pltpu.make_async_copy(OUT, out, hbm_sem.at[NLOADS]).wait()
    assert len(recv.at) == NSEM_RECV and len(sent.at) == NSEM_SEND and len(loads) == NLOADS


def per_device(
    tokens, gain_one, w_gate, w_up, w_down, scale_gate, scale_up, scale_down, gain_mix,
    w_query, w_key, w_value, w_outgate, scale_query, scale_key, scale_value, scale_outgate,
    ret_gain, decay_rate, w_mix, scale_mix, gain_two,
):
    freq = (1.0 / 10000.0 ** np.linspace(0.0, 1.0, 128)).astype(np.float32)
    angles = (np.arange(LEN, dtype=np.float32)[:, None] * np.repeat(freq, 2)[None, :]).astype(np.float64)
    cos_t = jnp.asarray(np.cos(angles), F32)
    sin_t = jnp.asarray(np.sin(angles), F32)
    row = lambda v: v.reshape(1, -1)
    small = [
        row(gain_one), row(gain_mix), row(gain_two), scale_gate, scale_up, row(scale_down), row(scale_query),
        row(scale_key), row(scale_value), row(scale_outgate), row(ret_gain), decay_rate, row(scale_mix),
    ]
    anywhere = pl.BlockSpec(memory_space=pl.ANY)
    vmem = pl.BlockSpec(memory_space=pltpu.VMEM)
    V = pltpu.VMEM
    hops = 3 * CHUNKS
    return pl.pallas_call(
        layer_kernel,
        out_shape=jax.ShapeDtypeStruct((CHUNKS * ROWS, 256), BF16),
        in_specs=[anywhere] * 11 + [vmem] * len(small),
        out_specs=anywhere,
        scratch_shapes=[
            V((2048, 768), BF16), V((384, 2048), BF16), V((2048, 1024), BF16), V((256, 2048), BF16),
            V((2, 128, 384), F32), V((384, 128), F32), V((4, 128, 256), F32), V((256, 128), F32),
            V((2, LEN, 256), F32), V((LEN, LEN), F32), V((8, 8, 256), F32),
            V((hops, 8, ROWS, 256), BF16), V((CHUNKS, ROWS, D), BF16), V((CHUNKS, ROWS, 384), BF16),
            V((CHUNKS, ROWS, 256), BF16), V((CHUNKS, ROWS, 256), BF16), V((CHUNKS * ROWS // LEN, LEN, 256), BF16),
            V((CHUNKS * ROWS // LEN, LEN, 256), BF16), V((CHUNKS, ROWS, 256), BF16), V((CHUNKS, 4, ROWS, 256), F32),
            V((hops, 4, ROWS, 256), BF16), V((hops, 4, ROWS, 256), BF16), V((hops, 3, ROWS, 256), BF16),
            V((hops, 2, HALF, 256), BF16), V((hops, 2, ROWS, 256), BF16), V((CHUNKS * ROWS, 256), BF16),
            pltpu.SemaphoreType.DMA((NLOADS + 1,)), pltpu.SemaphoreType.DMA((NSEM_RECV,)), pltpu.SemaphoreType.DMA((NSEM_SEND,)),
        ],
        compiler_params=pltpu.CompilerParams(
            collective_id=0, has_side_effects=True, vmem_limit_bytes=60 * 1024 * 1024
        ),
        name="layer",
    )(tokens, w_gate, w_up, w_down, w_query, w_key, w_value, w_outgate, w_mix, cos_t, sin_t, *small)


def solution(mesh):
    return jax.shard_map(
        per_device,
        mesh=mesh,
        in_specs=(
            P("fs", "tp"), P("tp"), P("fs", "tp"), P("fs", "tp"), P("tp", "fs"), P("tp"), P("tp"), P("tp"), P("tp"),
            P("fs", "tp"), P("fs", "tp"), P("fs", "tp"), P("fs", "tp"), P("tp"), P("tp"), P("tp"), P("tp"), P("tp"),
            P("tp"), P("tp", "fs"), P("tp"), P("tp"),
        ),
        out_specs=P("fs", "tp"),
        check_vma=False,
    )
```

```python
import functools

import jax
import jax.numpy as jnp
import numpy as np
from jax import lax
from jax.experimental import pallas as pl
from jax.experimental.pallas import tpu as pltpu
from jax.sharding import PartitionSpec as P

MESH = pl.DeviceIdType.MESH
BF16 = jnp.bfloat16
F32 = jnp.float32

D = 2048
LEN = 256
ROWS = 128
HALF = ROWS // 2
CHUNKS = 6
EPS = 1e-06
HEAD_EPS = 0.1
GROUPS = ("gu", "dn", "qk", "mx")
PIECE_ROWS = {"gu": 128, "dn": 384, "qk": 128, "mx": 256}
PIECE_BYTES = {"gu": 196608, "dn": 98304, "qk": 262144, "mx": 65536}
BLOCK = ROWS * 512


class Step:
    def __init__(self, run, waits=(), sends=(), needs=(), gives=None, cost=0.02, rank=1.0):
        self.run, self.waits, self.sends = run, waits, sends
        self.needs, self.gives, self.cost, self.rank = needs, gives, cost, rank


START = 0.7
MARGIN = 0.1
LATENCY = 2.6
PARTNER = 1.7
WAYS = ("x+", "x-", "d", "y+", "y-", "z+", "z-")
GROUP_BASE = (5.25, 5.75, 7.25, 9.25)
WPRI = (-0.5, -1.0, -13.75, -2.5, 0.25)
XPRI = (0.25, -3.75, 1.25, -1.0, 2.75, -11.5)
RANKS = (26.5, 0.45)
STAGE_GAP = 10.0
COST = {"norm": 0.37, "gu": 0.73, "qk": 0.83, "ret": 0.4, "dn": 0.32, "mx": 0.25}
GATE = (None, None, None)


def link_time(way, size):
    return size / (300e3 if way == "d" else 45.7e3)


def in_order(lists):
    clock, free, given, order = 0.0, {}, set(), []
    arrive = {"hbm": 0.3}
    for way in WAYS:
        free[way] = START
    pending = {way: [] for way in WAYS}
    heads = [0] * len(lists)
    count = 0

    def issue(way, entry):
        _, _, size, key, step, which = entry
        done = max(free[way], clock) + link_time(way, size)
        free[way] = done
        arrive[key] = max(arrive.get(key, 0.0), done + (PARTNER if way == "d" else LATENCY))
        missing[key] -= 1
        order.append((clock, step, which))

    missing = {"hbm": 0}
    for steps in lists:
        for step in steps:
            for _, _, key, _ in step.sends:
                missing[key] = missing.get(key, 0) + 1

    while True:
        best = None
        for number, steps in enumerate(lists):
            if heads[number] == len(steps):
                continue
            step = steps[heads[number]]
            if any(k not in given for k in step.needs) or any(missing[k] for k in step.waits):
                continue
            ready = max([clock] + [arrive[k] for k in step.waits])
            score = (ready, step.rank, number)
            if best is None or score < best[0]:
                best = (score, number, step)
        horizon = 1e9 if best is None else best[0][0] + best[2].cost + MARGIN
        issued = False
        for way in WAYS:
            if pending[way] and (way == "d" or free[way] < horizon):
                pending[way].sort(key=lambda e: e[:2])
                issue(way, pending[way].pop(0))
                issued = True
        if issued:
            continue
        if best is None:
            break
        (ready, _, _), number, step = best
        heads[number] += 1
        clock = ready + step.cost
        if step.gives is not None:
            given.add(step.gives)
        order.append((clock, step, None))
        for which, (way, size, key, urgency) in enumerate(step.sends):
            pending[way].append((urgency, count, size, key, step, which))
            count += 1
    assert all(h == len(s) for h, s in zip(heads, lists))
    return order


class Sems:
    def __init__(self, ref):
        self.ref, self.at = ref, {}

    def __getitem__(self, key):
        if key not in self.at:
            self.at[key] = len(self.at)
        return self.ref.at[self.at[key]]


NSEM_RECV = 103
NSEM_SEND = 11
NLOADS = 11


def layer_kernel(
    tokens, w_gate, w_up, w_down, w_query, w_key, w_value, w_outgate, w_mix, cos_t, sin_t,
    gain_one, gain_mix, gain_two, s_gate, s_up, s_down, s_query, s_key, s_value, s_outgate,
    ret_gain, decay, s_mix,
    out,
    W_gu, W_dn, W_qk, W_mx,
    F_gu, F_dn, F_qk, F_mx,
    TURN, DEC, GB, XG, NX, HID, QB, OG, KB, VB, MX, OB, PB, RD, SB, R1, FIN, OUT,
    hbm_sem, recv_sem, send_sem,
):
    fs, tp = lax.axis_index("fs"), lax.axis_index("tp")
    z, y = fs // 4, fs % 4
    x, c = tp // 2, tp % 2

    def around(v, k):
        return (v + k) % 4

    def fs_of(zz, yy):
        return zz * 4 + yy

    def tp_of(k, core):
        return around(x, k) * 2 + core

    where = {
        "x+": (fs, tp_of(1, c)), "x-": (fs, tp_of(3, c)), "d": (fs, x * 2 + (1 - c)),
        "y+": (fs_of(z, around(y, 1)), tp), "y-": (fs_of(z, around(y, 3)), tp),
        "z+": (fs_of(around(z, 1), y), tp), "z-": (fs_of(around(z, 3), y), tp),
    }
    W = {"gu": W_gu, "dn": W_dn, "qk": W_qk, "mx": W_mx}
    recv, sent = Sems(recv_sem), Sems(send_sem)

    def copy(src, dst, send_key, recv_key, way):
        return pltpu.make_async_remote_copy(
            src_ref=src, dst_ref=dst, send_sem=sent[send_key], recv_sem=recv[recv_key],
            device_id=where[way], device_id_type=MESH,
        )

    held = []

    def send(ref, send_key, recv_key, way, dst=None):
        held.append((way, lambda: copy(ref, ref if dst is None else dst, send_key, recv_key, way).start()))

    def got(ref, send_key, recv_key):
        copy(ref, ref, send_key, recv_key, "d").wait_recv()

    def left(ref, send_key, recv_key):
        copy(ref, ref, send_key, recv_key, "d").wait_send()

    loads = {}

    def load(key, src, dst):
        loads[key] = pltpu.make_async_copy(src, dst, hbm_sem.at[len(loads)])
        loads[key].start()

    def load_all(key, sources, dst):
        at = len(loads)
        loads[key] = pltpu.make_async_copy(dst, dst, hbm_sem.at[at])
        for n, src in enumerate(sources):
            pltpu.make_async_copy(src, dst.at[n], hbm_sem.at[at]).start()

    load_all("gu", (w_gate, w_up), F_gu)
    for k in range(CHUNKS):
        load(("t", k), tokens.at[pl.ds(k * ROWS, ROWS), :], XG.at[k, tp])
    load("d", w_down, F_dn)
    load_all("q", (w_query, w_key, w_value, w_outgate), F_qk)
    load("m", w_mix, F_mx)
    load_all("turn", (cos_t, sin_t), TURN)

    barrier = pltpu.get_barrier_semaphore()
    for way in WAYS:
        pl.semaphore_signal(barrier, inc=1, device_id=where[way], device_id_type=MESH)

    lists = []

    def wpart(g, f, half, quarter=None):
        n = PIECE_ROWS[g] // 2
        lo = n * half
        if quarter is not None:
            n //= 2
            lo += n * quarter
        if g in ("gu", "qk"):
            return W[g].at[pl.ds(pl.multiple_of(f * 128 + lo, 32), n), :]
        return W[g].at[pl.ds(lo, n), pl.ds(pl.multiple_of(f * 128, 128), 128)]

    def wspan(g, pieces):
        if g in ("gu", "qk"):
            return W[g].at[pl.ds(0, 128 * pieces), :]
        return W[g].at[:, pl.ds(0, 128 * pieces)]

    def cast_gu():
        loads["gu"].wait()
        rows = pl.ds(pl.multiple_of(fs * 128, 128), 128)
        for j in range(3):
            W_gu[rows, 256 * j : 256 * j + 128] = F_gu[0, :, 128 * j : 128 * j + 128].astype(BF16)
            W_gu[rows, 256 * j + 128 : 256 * j + 256] = F_gu[1, :, 128 * j : 128 * j + 128].astype(BF16)

    def cast_dn():
        loads["d"].wait()
        W_dn[:, pl.ds(pl.multiple_of(fs * 128, 128), 128)] = F_dn[...].astype(BF16)

    def cast_qk():
        rows = pl.ds(pl.multiple_of(fs * 128, 128), 128)
        loads["q"].wait()
        for n in range(4):
            W_qk[rows, 256 * n : 256 * n + 256] = F_qk[n].astype(BF16)

    def cast_mx():
        loads["m"].wait()
        W_mx[:, pl.ds(pl.multiple_of(fs * 128, 128), 128)] = F_mx[...].astype(BF16)

    casts = {"gu": cast_gu, "dn": cast_dn, "qk": cast_qk, "mx": cast_mx}
    cast_steps = []
    for n, g in enumerate(GROUPS):
        cast_steps.append(Step(casts[g], waits=("hbm",), gives=("cast", g), cost=0.05, rank=-5 if n == 0 else 1.5))
    lists.append(cast_steps)

    def weight_lists(order, g):
        rank = RANKS[1] + 0.1 * order
        base = GROUP_BASE[order]
        for half in (0, 1):
            a, b = ("y", "z") if half == 0 else ("z", "y")

            def at(i, j, a=a):
                return fs_of(around(z, j), around(y, i)) if a == "y" else fs_of(around(z, i), around(y, j))

            full = PIECE_BYTES[g] // 2
            key = lambda *k, half=half: ("w", g, half) + k
            skey = ("w", g)

            def both(i, half=half, at=at, a=a, b=b, key=key, full=full):
                def run():
                    for way in (b + "+", b + "-"):
                        send(wpart(g, at(i, 0), half), skey, key("s", i), way)
                return run, [(way, full, key("s", i), base + WPRI[3 if i else 1]) for way in (b + "+", b + "-")]

            def own(half=half, at=at, a=a, b=b, key=key, full=full):
                more, extra = both(0)
                def run():
                    for way in (a + "+", a + "-"):
                        send(wpart(g, at(0, 0), half), skey, key("f"), way)
                    more()
                return run, [(way, full, key("f"), base + WPRI[0]) for way in (a + "+", a + "-")] + extra

            def first(half=half, at=at, a=a, b=b, key=key, full=full):
                (one, extra_one), (two, extra_two) = both(3), both(1)
                def run():
                    got(wspan(g, 1), skey, key("f"))
                    for i, back, q in ((3, "+", 0), (1, "-", 1)):
                        send(wpart(g, at(i, 0), half, q), skey, key("f2"), a + back)
                    one()
                    two()
                return run, [(a + back, full // 2, key("f2"), base + WPRI[2]) for back in "+-"] + extra_one + extra_two

            def far(half=half, at=at, a=a, b=b, key=key):
                more, extra = both(2)
                def run():
                    got(wpart(g, at(2, 0), half), skey, key("f2"))
                    more()
                return run, extra

            def second(i, half=half, at=at, a=a, b=b, key=key, full=full):
                def run():
                    got(wspan(g, 1), skey, key("s", i))
                    for j, back, q in ((3, "+", 0), (1, "-", 1)):
                        send(wpart(g, at(i, j), half, q), skey, ("w", g, "end"), b + back)
                return run, [(b + back, full // 2, ("w", g, "end"), base + WPRI[4]) for back in "+-"]

            run, sends = own()
            needs = [("cast", g)]
            if order and GATE[order - 1]:
                needs += [(GATE[order - 1], GROUPS[order - 1], h) for h in (0, 1)]
            steps = [Step(run, sends=sends, needs=needs, gives=("own", g, half), rank=rank)]
            run, sends = first()
            steps.append(Step(run, waits=(key("f"),), sends=sends, rank=rank, gives=("near", g, half)))
            run, sends = far()
            steps.append(Step(run, waits=(key("f2"),), sends=sends, rank=rank, gives=("far", g, half)))
            lists.append(steps)
            steps = []
            for i in (0, 3, 1, 2):
                run, sends = second(i)
                steps.append(Step(run, waits=(key("s", i),), sends=sends, rank=rank))
            steps[-1].gives = ("last", g, half)
            lists.append(steps)

        def end():
            got(wspan(g, 4), ("w", g), ("w", g, "end"))
        lists.append([Step(end, waits=(("w", g, "end"),), needs=(("last", g, 0), ("last", g, 1)), gives=("W", g), rank=rank)])

    for order, g in enumerate(GROUPS):
        weight_lists(order, g)

    def tables():
        loads["turn"].wait()
        n = lax.broadcasted_iota(jnp.int32, (LEN, LEN), 0)
        m = lax.broadcasted_iota(jnp.int32, (LEN, LEN), 1)
        distance = jnp.maximum(n - m, 0).astype(F32)
        DEC[...] = jnp.where(n >= m, jnp.exp(-decay[...].reshape(1, 1) * distance), 0.0) * (LEN ** -0.5)

    lists.append([Step(tables, waits=("hbm",), gives="tables", rank=3.0, cost=0.15)])

    def chunk_list(k):
        steps = []
        base = 0.0 + 0.01 * k
        seq, half = k * ROWS // LEN, k % (LEN // ROWS)

        for s in range(3):
            n = s * CHUNKS + k
            xg = XG.at[n]
            akey, rkey = ("a", n), ("r", n)
            acode, rcode, asend, rsend = ("a", k), ("r", k), ("as", s), ("rs", s)

            def slot(t, n=n):
                return XG.at[n, t]

            def half_of(t, h, n=n):
                return XG.at[n, t, pl.ds(HALF * h, HALF), :]

            gains = s == 0 and k == 0

            def a0(s=s, akey=acode, asend=asend, slot=slot, gains=gains):
                if s == 0:
                    loads[("t", k)].wait()
                for way, r in (("x+", "L"), ("x-", "L"), ("d", "D")):
                    send(slot(tp), asend, akey + (r,), way)
                if gains:
                    for i, gain in enumerate((gain_one, gain_mix, gain_two)):
                        GB[tp, i : i + 1, :] = gain[...]
                    for way, r in (("x+", "L"), ("x-", "L"), ("d", "D")):
                        send(GB.at[tp], ("g",), ("g", r), way)

            def a1(akey=acode, asend=asend, slot=slot, half_of=half_of, n=n, gains=gains):
                got(XG.at[n, pl.ds(0, 2)], asend, akey + ("L",))
                before, after = tp_of(3, c), tp_of(1, c)
                send(half_of(before, 0), asend, akey + ("F",), "x+")
                send(half_of(after, 1), asend, akey + ("F",), "x-")
                send(slot(before), asend, akey + ("D",), "d")
                send(slot(after), asend, akey + ("D",), "d")
                if gains:
                    got(GB.at[pl.ds(0, 2)], ("g",), ("g", "L"))
                    send(GB.at[before], ("g",), ("g", "F"), "x+")
                    send(GB.at[before], ("g",), ("g", "D"), "d")
                    send(GB.at[after], ("g",), ("g", "D"), "d")

            def a3(akey=acode, asend=asend, slot=slot, gains=gains):
                t = tp_of(2, c)
                got(slot(t), asend, akey + ("F",))
                send(slot(t), asend, akey + ("D",), "d")
                if gains:
                    got(GB.at[t], ("g",), ("g", "F"))
                    send(GB.at[t], ("g",), ("g", "D"), "d")

            def normed(n=n, s=s, akey=acode, asend=asend, gains=gains):
                got(XG.at[n, pl.ds(0, 4)], asend, akey + ("D",))
                if gains:
                    got(GB.at[pl.ds(0, 4)], ("g",), ("g", "D"))

                def rows_of(i, carry):
                    r = pl.ds(pl.multiple_of(i * 16, 16), 16)
                    hs = [XG[n, t, r, :].astype(F32) for t in range(8)]
                    squares = hs[0] * hs[0]
                    for h in hs[1:]:
                        squares += h * h
                    scale = lax.rsqrt(jnp.sum(squares, axis=1, keepdims=True) / D + EPS)
                    for t in range(8):
                        NX[k, r, 256 * t : 256 * t + 256] = (hs[t] * scale * GB[t, s : s + 1, :]).astype(BF16)
                    return carry

                lax.fori_loop(0, ROWS // 16, rows_of, 0, unroll=8)

            def gate_up():
                for j in range(3):
                    both = jnp.dot(NX[k], W_gu[:, 256 * j : 256 * j + 256], preferred_element_type=F32)
                    lane = slice(128 * j, 128 * j + 128)
                    gate = both[:, :128] * s_gate[lane].reshape(1, 128)
                    up = both[:, 128:] * s_up[lane].reshape(1, 128)
                    HID[k, :, lane] = (gate / (1.0 + jnp.exp(-gate)) * up).astype(BF16)

            def turned(v):
                at = slice(ROWS * half, ROWS * half + ROWS)
                even = lax.broadcasted_iota(jnp.int32, (ROWS, 256), 1) % 2 == 0
                swapped = jnp.where(even, -pltpu.roll(v, 255, 1), pltpu.roll(v, 1, 1))
                return (v * TURN[0, at, :] + swapped * TURN[1, at, :]).astype(BF16)

            def query_key():
                at = slice(ROWS * half, ROWS * half + ROWS)
                for j, scale in enumerate((s_key, s_value, s_query, s_outgate)):
                    col = 256 * (1, 2, 0, 3)[j]
                    pre = jnp.dot(NX[k], W_qk[:, col : col + 256], preferred_element_type=F32)
                    row = (pre * scale[...]).astype(BF16)
                    if j == 0:
                        KB[seq, at, :] = turned(row.astype(F32))
                    elif j == 1:
                        VB[seq, at, :] = row
                    elif j == 2:
                        QB[k] = turned(row.astype(F32))
                    else:
                        OG[k] = row

            def retained():
                seen = ROWS * half + ROWS
                scores = lax.dot_general(
                    QB[k], KB[seq, 0:seen, :], (((1,), (1,)), ((), ())), preferred_element_type=F32
                )
                scores = scores * DEC[ROWS * half : seen, 0:seen]
                kept = jnp.dot(scores.astype(BF16), VB[seq, 0:seen, :], preferred_element_type=F32)
                kept = kept * lax.rsqrt(jnp.mean(kept * kept, axis=1, keepdims=True) + HEAD_EPS)
                gate = OG[k].astype(F32)
                MX[k] = (kept * ret_gain[...] * (gate / (1.0 + jnp.exp(-gate)))).astype(BF16)

            def product(i, core, s=s):
                cols = pl.ds(pl.multiple_of((around(x, i) * 2 + core) * 256, 256), 256)
                if s == 1:
                    return jnp.dot(MX[k], W_mx[:, cols], preferred_element_type=F32)
                return jnp.dot(HID[k], W_dn[:, cols], preferred_element_type=F32)

            def theirs(n=n, rkey=rcode, rsend=rsend, product=product):
                for i, r in ((2, "2"), (1, "13"), (3, "13"), (0, "0")):
                    PB[n, i] = product(i, 1 - c).astype(BF16)
                    send(PB.at[n, i], rsend, rkey + (r,), "d", RD.at[n, i])

            def mine(product=product):
                for i in (2, 1, 3, 0):
                    OB[k, i] = product(i, c)

            def r0(n=n, rkey=rcode, rsend=rsend):
                got(RD.at[n, 2], rsend, rkey + ("2",))
                SB[n, 0] = (OB[k, 2] + RD[n, 2].astype(F32)).astype(BF16)
                send(SB.at[n, 0, pl.ds(0, HALF)], rsend, rkey + ("L",), "x+", R1.at[n, 0])
                send(SB.at[n, 0, pl.ds(HALF, HALF)], rsend, rkey + ("L",), "x-", R1.at[n, 1])

            def r1(n=n, rkey=rcode, rsend=rsend):
                got(RD.at[n, pl.ds(0, 2)], rsend, rkey + ("13",))
                upper = OB[k, 1, HALF:ROWS] + RD[n, 1, HALF:ROWS].astype(F32)
                SB[n, 1, HALF:ROWS] = upper.astype(BF16)
                send(SB.at[n, 1, pl.ds(HALF, HALF)], rsend, rkey + ("E",), "x+", FIN.at[n, 0, pl.ds(HALF, HALF)])
                lower = OB[k, 3, 0:HALF] + RD[n, 3, 0:HALF].astype(F32)
                SB[n, 2, 0:HALF] = lower.astype(BF16)
                send(SB.at[n, 2, pl.ds(0, HALF)], rsend, rkey + ("E",), "x-", FIN.at[n, 1, pl.ds(0, HALF)])

            def r2(n=n, rkey=rcode, rsend=rsend):
                got(R1.at[n], rsend, rkey + ("L",))
                SB[n, 1, 0:HALF] = (
                    OB[k, 1, 0:HALF] + RD[n, 1, 0:HALF].astype(F32) + R1[n, 0].astype(F32)
                ).astype(BF16)
                send(SB.at[n, 1, pl.ds(0, HALF)], rsend, rkey + ("E",), "x+", FIN.at[n, 0, pl.ds(0, HALF)])
                SB[n, 2, HALF:ROWS] = (
                    OB[k, 3, HALF:ROWS] + RD[n, 3, HALF:ROWS].astype(F32) + R1[n, 1].astype(F32)
                ).astype(BF16)
                send(SB.at[n, 2, pl.ds(HALF, HALF)], rsend, rkey + ("E",), "x-", FIN.at[n, 1, pl.ds(HALF, HALF)])

            def r4(n=n, s=s, rkey=rcode, rsend=rsend):
                got(RD.at[n, 0], rsend, rkey + ("0",))
                got(FIN.at[n], rsend, rkey + ("E",))
                total = OB[k, 0] + RD[n, 0].astype(F32) + FIN[n, 0].astype(F32) + FIN[n, 1].astype(F32)
                if s == 1:
                    total = total * s_mix[...]
                else:
                    total = 0.5 * total * s_down[...]
                after = (XG[n, tp].astype(F32) + total).astype(BF16)
                if s < 2:
                    XG[n + CHUNKS, tp] = after
                else:
                    OUT[k * ROWS : k * ROWS + ROWS, :] = after
                    rows = pl.ds(k * ROWS, ROWS)
                    pltpu.make_async_copy(OUT.at[rows, :], out.at[rows, :], hbm_sem.at[NLOADS]).start()

            ua, ur = 2 * s * STAGE_GAP + k, (2 * s + 1) * STAGE_GAP + k
            base = 0.01 * ua
            L, F, Dk = (akey + (r,) for r in "LFD")
            extra = {r: ("g", r) for r in "LFD"}
            sends = [("x+", BLOCK, L, ua + XPRI[0]), ("x-", BLOCK, L, ua + XPRI[0]), ("d", BLOCK, Dk, ua)]
            waits = ("hbm",) if s == 0 else ()
            add = lambda *pairs: [(w, 8192, extra[q], -9) for w, q in pairs] if gains else []
            more = lambda q: (extra[q],) if gains else ()
            steps.append(Step(a0, waits=waits, sends=sends + add(("x+", "L"), ("x-", "L"), ("d", "D")),
                              rank=base + (0.0 if s else -1 + 0.1 * k)))
            sends = [("x+", BLOCK // 2, F, ua + XPRI[1]), ("x-", BLOCK // 2, F, ua + XPRI[1])] + 2 * [("d", BLOCK, Dk, ua)]
            steps.append(Step(a1, waits=(L,) + more("L"), sends=sends + add(("x+", "F"), ("d", "D"), ("d", "D")), rank=base))
            steps.append(Step(a3, waits=(F,) + more("F"), sends=[("d", BLOCK, Dk, ua)] + add(("d", "D")), rank=base))
            needs = ("gains",) if s == 0 and k else ()
            steps.append(Step(normed, waits=(Dk,) + more("D"), needs=needs, gives="gains" if gains else None,
                              rank=RANKS[0] + base, cost=COST["norm"]))
            if s == 1:
                steps.append(Step(query_key, needs=(("W", "qk"), "tables"), rank=RANKS[0] + base, cost=COST["qk"], gives=("kv", k)))
                steps.append(Step(retained, needs=tuple(("kv", k - i) for i in range(half + 1)), rank=RANKS[0] + base, cost=COST["ret"]))
                end, cost = ("W", "mx"), COST["mx"]
            else:
                steps.append(Step(gate_up, needs=(("W", "gu"),), rank=RANKS[0] + base, cost=COST["gu"]))
                end, cost = ("W", "dn"), COST["dn"]
            r = lambda q: rkey + (q,)
            steps.append(Step(theirs, needs=(end,), rank=RANKS[0] + base, cost=cost,
                              sends=[("d", BLOCK, r(q), ur) for q in ("2", "13", "13", "0")]))
            steps.append(Step(mine, rank=RANKS[0] + base, cost=cost))
            two = lambda q, i: [(w, BLOCK // 2, r(q), ur + XPRI[i]) for w in ("x+", "x-")]
            steps.append(Step(r0, waits=(r("2"),), rank=base, sends=two("L", 2), cost=0.03))
            steps.append(Step(r1, waits=(r("13"),), rank=base, sends=two("E", 3), cost=0.03))
            steps.append(Step(r2, waits=(r("L"),), rank=base, sends=two("E", 4), cost=0.05))
            steps.append(Step(r4, waits=(r("E"), r("0")), rank=base, cost=0.1))
        return steps

    for k in range(CHUNKS):
        lists.append(chunk_list(k))

    order = in_order(lists)
    pl.semaphore_wait(barrier, 7)
    for _, step, which in order:
        if which is None:
            held.clear()
            step.run()
            step.held = list(held)
            assert [w for w, _ in held] == [e[0] for e in step.sends]
        else:
            step.held[which][1]()

    for g in GROUPS:
        left(wspan(g, 15), ("w", g), ("w", g, "end"))
    left(GB.at[pl.ds(0, 7)], ("g",), ("g", "D"))
    for s in range(3):
        left(XG.at[pl.ds(0, CHUNKS), pl.ds(0, 7)], ("as", s), ("a", 0, "D"))
        left(XG.at[pl.ds(0, CHUNKS), pl.ds(0, 7)], ("rs", s), ("r", 0, "0"))
    pltpu.make_async_copy(OUT, out, hbm_sem.at[NLOADS]).wait()
    assert len(recv.at) == NSEM_RECV and len(sent.at) == NSEM_SEND and len(loads) == NLOADS


def per_device(
    tokens, gain_one, w_gate, w_up, w_down, scale_gate, scale_up, scale_down, gain_mix,
    w_query, w_key, w_value, w_outgate, scale_query, scale_key, scale_value, scale_outgate,
    ret_gain, decay_rate, w_mix, scale_mix, gain_two,
):
    freq = (1.0 / 10000.0 ** np.linspace(0.0, 1.0, 128)).astype(np.float32)
    angles = (np.arange(LEN, dtype=np.float32)[:, None] * np.repeat(freq, 2)[None, :]).astype(np.float64)
    cos_t = jnp.asarray(np.cos(angles), F32)
    sin_t = jnp.asarray(np.sin(angles), F32)
    row = lambda v: v.reshape(1, -1)
    small = [
        row(gain_one), row(gain_mix), row(gain_two), scale_gate, scale_up, row(scale_down), row(scale_query),
        row(scale_key), row(scale_value), row(scale_outgate), row(ret_gain), decay_rate, row(scale_mix),
    ]
    anywhere = pl.BlockSpec(memory_space=pl.ANY)
    vmem = pl.BlockSpec(memory_space=pltpu.VMEM)
    V = pltpu.VMEM
    hops = 3 * CHUNKS
    return pl.pallas_call(
        layer_kernel,
        out_shape=jax.ShapeDtypeStruct((CHUNKS * ROWS, 256), BF16),
        in_specs=[anywhere] * 11 + [vmem] * len(small),
        out_specs=anywhere,
        scratch_shapes=[
            V((2048, 768), BF16), V((384, 2048), BF16), V((2048, 1024), BF16), V((256, 2048), BF16),
            V((2, 128, 384), F32), V((384, 128), F32), V((4, 128, 256), F32), V((256, 128), F32),
            V((2, LEN, 256), F32), V((LEN, LEN), F32), V((8, 8, 256), F32),
            V((hops, 8, ROWS, 256), BF16), V((CHUNKS, ROWS, D), BF16), V((CHUNKS, ROWS, 384), BF16),
            V((CHUNKS, ROWS, 256), BF16), V((CHUNKS, ROWS, 256), BF16), V((CHUNKS * ROWS // LEN, LEN, 256), BF16),
            V((CHUNKS * ROWS // LEN, LEN, 256), BF16), V((CHUNKS, ROWS, 256), BF16), V((CHUNKS, 4, ROWS, 256), F32),
            V((hops, 4, ROWS, 256), BF16), V((hops, 4, ROWS, 256), BF16), V((hops, 3, ROWS, 256), BF16),
            V((hops, 2, HALF, 256), BF16), V((hops, 2, ROWS, 256), BF16), V((CHUNKS * ROWS, 256), BF16),
            pltpu.SemaphoreType.DMA((NLOADS + 1,)), pltpu.SemaphoreType.DMA((NSEM_RECV,)), pltpu.SemaphoreType.DMA((NSEM_SEND,)),
        ],
        compiler_params=pltpu.CompilerParams(
            collective_id=0, has_side_effects=True, vmem_limit_bytes=60 * 1024 * 1024
        ),
        name="layer",
    )(tokens, w_gate, w_up, w_down, w_query, w_key, w_value, w_outgate, w_mix, cos_t, sin_t, *small)


def solution(mesh):
    return jax.shard_map(
        per_device,
        mesh=mesh,
        in_specs=(
            P("fs", "tp"), P("tp"), P("fs", "tp"), P("fs", "tp"), P("tp", "fs"), P("tp"), P("tp"), P("tp"), P("tp"),
            P("fs", "tp"), P("fs", "tp"), P("fs", "tp"), P("fs", "tp"), P("tp"), P("tp"), P("tp"), P("tp"), P("tp"),
            P("tp"), P("tp", "fs"), P("tp"), P("tp"),
        ),
        out_specs=P("fs", "tp"),
        check_vma=False,
    )
```
